256 devices in a mesh: ep: 64 (over z, x, core), tp: 4 (over y).
Axes of the slice: x: 4, y: 4, z: 8, core: 2. Of those that a mesh axis runs over, the one named last changes fastest.
Arguments:
- mixer_input: bfloat16 [32768, 2048], P('ep'), may hold values from -5.5 to 5.5
- expert_input: bfloat16 [32768, 2048], P('ep'), may hold values from -6 to 6
- gain_mixer: float32 [2048], replicated, may hold values from 0.1 to 1.9
- gain_expert: float32 [2048], replicated, may hold values from 0.1 to 1.9
- query_weight: bfloat16 [2048, 1536], P(None, 'tp')
- key_weight: bfloat16 [2048, 256], P(None, 'tp')
- value_weight: bfloat16 [2048, 256], P(None, 'tp'), may hold values from -0.125 to 0.125
- sink_logits: float32 [24], P('tp'), may hold values from 2 to 6
- output_weight: bfloat16 [1536, 2048], P('tp'), may hold values from -0.75 to 0.75
- expert_choice: int32 [32768, 2], P('ep'), may hold values from 0 to 63, all different within a row; in each aligned block of 128 rows (0 to 127, 128 to 255, ...) at most 8 rows name the same one
- route_weights: float32 [32768, 2], P('ep'), may hold values from 0.2 to 1.2
- expert_gate: bfloat16 [64, 2048, 1024], P('ep', None, 'tp'), may hold values from -0.125 to 0.125
- expert_up: bfloat16 [64, 2048, 1024], P('ep', None, 'tp'), may hold values from -0.125 to 0.125
- expert_down: bfloat16 [64, 1024, 2048], P('ep', 'tp'), may hold values from -0.1875 to 0.1875
- shared_gate: bfloat16 [2048, 512], P(None, 'tp'), may hold values from -0.125 to 0.125
- shared_up: bfloat16 [2048, 512], P(None, 'tp'), may hold values from -0.125 to 0.125
- shared_down: bfloat16 [512, 2048], P('tp'), may hold values from -0.25 to 0.25
Outputs:
- mixer_output: bfloat16 [32768, 2048], P(('ep', 'tp'))
- expert_output: bfloat16 [32768, 2048], P(('ep', 'tp'))
The draws below stay inside these ranges and needn't reach their ends.
Inputs may be any that keep to these rules, and one draw needn't show every extreme that they name: `expert_choice`: in each aligned block of 128 rows no expert is named by more than 8 rows, and in some block some expert is named by exactly 8 rows; the 2 entries of a row differ.
All inputs are finite; a program needn't handle non-finite values.
Results may differ from the reference program's by a relative error of at most 0.019.
Values may be sent and summed in bfloat16 or wider, within the bound.
A program may use at most 128 MiB of HBM per device.

```python
import math
import jax
import jax.numpy as jnp
import numpy as np
from jax import lax

D = 2048
HEADS = 24
KV_HEADS = 4
HEAD_DIM = 64
WINDOW = 128
SEQS = 1
EXPERT_FF = 1024
SHARED_FF = 512
TOP = 2
TOK_B_DEV = 128
EXPERTS = 64
TOKENS_A = 32768
TOKENS_B = 32768
SEQ_LEN = 32768
CAP = 8
N_TP = 4


def attention_weights(key):
    base_key = jax.random.fold_in(key, 41)
    key_part = jax.random.truncated_normal(jax.random.fold_in(base_key, 1), -4.0, 4.0, (D, KV_HEADS * HEAD_DIM), jnp.float32) * D ** (-0.5)
    query_part = jax.random.truncated_normal(jax.random.fold_in(base_key, 2), -4.0, 4.0, (D, HEADS * HEAD_DIM), jnp.float32) * D ** (-0.5)
    return (key_part, query_part)


def draw_key_weight(key, part):
    key_part, query_part = attention_weights(key)
    return key_part.astype(jnp.bfloat16)


def draw_query_weight(key, part):
    key_part, query_part = attention_weights(key)
    return query_part.astype(jnp.bfloat16)


def draw_mixer_input(key, part):
    base_key = jax.random.fold_in(key, 53)
    values = jax.random.truncated_normal(jax.random.fold_in(base_key, 1), -5.0, 5.0, (TOKENS_A, D), jnp.float32)
    return values.astype(jnp.bfloat16)


def steps_of(stream_key, dims, pieces, low, largest):
    def one(axis_at, parts):
        draws = jax.random.uniform(jax.random.fold_in(jax.random.fold_in(stream_key, 6), axis_at), (parts,), jnp.float32, low / len(pieces), largest / len(pieces))
        return jnp.repeat(jnp.exp(draws), dims[axis_at] // parts).reshape((-1,) + (1,) * (len(dims) - axis_at - 1))

    loudness = one(*pieces[0])
    for cut in pieces[1:]:
        loudness = loudness * one(*cut)
    return loudness


def deal_out(stream_key, own, number, rows, amount, top, most, lean):
    ranking = jax.random.permutation(stream_key, amount)
    crowded, ordinary = shares(amount, rows * top, most, lean, True), shares(amount, rows * top, most, lean, False)
    places = jnp.arange(amount)

    def named(tallies, turn):
        used = int((tallies > 0).sum())
        fixed = max(1, used // 4)
        moved = fixed + (places - fixed + turn * (used - fixed)) % max(1, amount - fixed)
        return jnp.zeros((amount,), jnp.int32).at[ranking[jnp.where(places < fixed, places, moved)]].set(jnp.asarray(tallies, jnp.int32))

    tallies = jnp.where(number % 4 == 0, named(crowded, number // 4), named(ordinary, number - number // 4 - 1))
    mixed = jax.random.permutation(jax.random.fold_in(own, 3), amount)
    source_of, sink = mixed[0:amount // 2 * 2:2], mixed[1:amount // 2 * 2:2]
    margin = jnp.minimum(tallies[source_of] - 1, most - tallies[sink]) // 2
    margin = jnp.where((source_of == ranking[0]) | (sink == ranking[0]) | (tallies[sink] == 0), 0, jnp.maximum(margin, 0))
    moved = jax.random.randint(jax.random.fold_in(own, 4), (amount // 2,), 0, 1 << 20) % (margin + 1)
    tallies = tallies.at[source_of].add(-moved).at[sink].add(moved)
    items = jnp.searchsorted(jnp.cumsum(tallies), jnp.arange(rows * top), side="right").astype(jnp.int32)
    listing = items.reshape(top, rows).T
    listing = listing[jax.random.permutation(jax.random.fold_in(own, 1), rows)]
    turn = jax.random.randint(jax.random.fold_in(own, 2), (rows, 1), 0, top)
    return jnp.take_along_axis(listing, (jnp.arange(top)[None, :] + turn) % top, axis=1)


def shares(number_of, total, bound, skew, full):
    loads = [(1 << 20) // math.isqrt(grade ** skew) + 1 for grade in range(1, number_of + 1)]
    largest = bound if full else min(bound, max(-(-total // number_of), total * loads[0] // sum(loads)))
    least = 1 if total - largest >= number_of - 1 else 0
    counts, surplus = [largest] + [least] * (number_of - 1), total - largest - least * (number_of - 1)
    while surplus > 0:
        movable = [i for i in range(1, number_of) if counts[i] < largest] or [i for i in range(1, number_of) if counts[i] < bound]
        whole, remaining = sum([loads[i] for i in movable]), surplus
        for i in movable:
            more = min(bound - counts[i], max(1, remaining * loads[i] // whole), surplus)
            counts[i] = counts[i] + more
            surplus = surplus - more
    return np.array(counts)


def bell_draw(own_key, dims, scale, bound, pieces=(), kind=jnp.bfloat16):
    entries = jax.random.normal(own_key, dims, jnp.float32) * scale
    if len(pieces) > 0:
        entries = steps_of(own_key, dims, pieces, -0.22, 0.18) * entries
    return jnp.clip(entries, min=-bound, max=bound).astype(kind)


def setup_inputs(seed: int = 0) -> dict:
    key_of = jax.random.split(jax.random.key(seed), 18)
    mixer_input = draw_mixer_input(jax.random.fold_in(key_of[17], 71), 0)
    expert_input = bell_draw(key_of[1], (TOKENS_B, D), 1.0, 6.0, ((0, 64),))
    gain_mixer = jnp.clip(1.0 + 0.18 * jax.random.normal(key_of[2], (D,), jnp.float32), 0.1, 1.9)
    gain_expert = jnp.clip(1.0 + 0.18 * jax.random.normal(key_of[3], (D,), jnp.float32), 0.1, 1.9)
    query_weight = draw_query_weight(jax.random.fold_in(key_of[17], 71), 0)
    key_weight = draw_key_weight(jax.random.fold_in(key_of[17], 71), 0)
    value_weight = bell_draw(key_of[6], (D, KV_HEADS * HEAD_DIM), D ** -0.5, 0.125, ((1, 4),))
    sink_logits = jnp.clip(2.0 + 4.0 * jax.random.uniform(key_of[7], (HEADS,), jnp.float32) ** steps_of(key_of[7], (HEADS,), ((0, 4),), -0.2, 0.2), 2.0, 6.0)
    output_weight = bell_draw(key_of[8], (HEADS * HEAD_DIM, D), (HEADS * HEAD_DIM // 25) ** -0.5, 0.75, ((0, 4),))
    expert_choice_keys = jax.random.split(jax.random.fold_in(key_of[9], 1), TOKENS_B // TOK_B_DEV)
    expert_choice_turns = jax.random.permutation(jax.random.fold_in(key_of[9], 3), TOKENS_B // TOK_B_DEV)
    expert_choice = jax.vmap(lambda own, number: deal_out(jax.random.fold_in(key_of[9], 2), own, number, TOK_B_DEV, EXPERTS, TOP, CAP, 2))(expert_choice_keys, expert_choice_turns).reshape((TOKENS_B, TOP))
    route_weights = jnp.clip(0.2 + 1 * jax.random.uniform(key_of[10], (TOKENS_B, TOP), jnp.float32) ** steps_of(key_of[10], (TOKENS_B, TOP), ((0, 64),), -0.2, 0.2), 0.2, 1.2)
    expert_gate = bell_draw(key_of[11], (EXPERTS, D, EXPERT_FF), D ** -0.5, 0.125, ((0, 64), (2, 4)))
    expert_up = bell_draw(key_of[12], (EXPERTS, D, EXPERT_FF), D ** -0.5, 0.125, ((0, 64), (2, 4)))
    expert_down = bell_draw(key_of[13], (EXPERTS, EXPERT_FF, D), EXPERT_FF ** -0.5, 0.1875, ((0, 64), (1, 4)))
    shared_gate = bell_draw(key_of[14], (D, SHARED_FF), D ** -0.5, 0.125, ((1, 4),))
    shared_up = bell_draw(key_of[15], (D, SHARED_FF), D ** -0.5, 0.125, ((1, 4),))
    shared_down = bell_draw(key_of[16], (SHARED_FF, D), SHARED_FF ** -0.5, 0.25, ((0, 4),))
    return dict(mixer_input=mixer_input, expert_input=expert_input, gain_mixer=gain_mixer, gain_expert=gain_expert, query_weight=query_weight, key_weight=key_weight, value_weight=value_weight, sink_logits=sink_logits, output_weight=output_weight, expert_choice=expert_choice, route_weights=route_weights, expert_gate=expert_gate, expert_up=expert_up, expert_down=expert_down, shared_gate=shared_gate, shared_up=shared_up, shared_down=shared_down)


norm_eps = 1e-06
rope_base = 500000.0

def rounded(value):
    return lax.optimization_barrier(value.astype(jnp.bfloat16)).astype(jnp.float32)

def rms_scale(matrix, scaling):
    widened = matrix.astype(jnp.float32)
    scaled = widened * lax.rsqrt(lax.optimization_barrier(jnp.mean(widened * widened, axis=-1, keepdims=True)) + norm_eps)
    return (scaled * scaling).astype(jnp.bfloat16)

def frequencies(head_size):
    half_steps = jnp.arange(head_size // 2, dtype=jnp.float32)
    return rope_base ** (-(2.0 * half_steps) / head_size)

def rotate(heads, angles):
    middle = heads.shape[-1] // 2
    widened = heads.astype(jnp.float32)
    cosine = jnp.cos(angles)[:, None, :]
    sine_val = jnp.sin(angles)[:, None, :]
    leading = widened[..., :middle]
    trailing = widened[..., middle:]
    turned = jnp.concatenate([leading * cosine - trailing * sine_val, trailing * cosine + leading * sine_val], axis=-1)
    return turned.astype(jnp.bfloat16)

def attend(query_heads, key_heads, value_heads, prior_keys, prior_values, first_position, sink_logits):
    window = prior_keys.shape[0]
    total_rows, kv_count, head_size = key_heads.shape
    group_size = query_heads.shape[1] // kv_count
    blocks = total_rows // window

    def banded(earlier, current):
        joined = jnp.concatenate([earlier, current], axis=0).reshape(blocks + 1, window, kv_count, head_size)
        return jnp.concatenate([joined[:-1], joined[1:]], axis=1)
    band_keys = banded(prior_keys, key_heads)
    band_values = banded(prior_values, value_heads)
    query_blocks = query_heads.reshape(blocks, window, kv_count, group_size, head_size)
    scores = jnp.einsum('nqhgd,nkhd->nhgqk', query_blocks.astype(jnp.float32), band_keys.astype(jnp.float32)) / math.sqrt(head_size)
    query_index = jnp.arange(window, dtype=jnp.int32)[:, None]
    key_index = jnp.arange(2 * window, dtype=jnp.int32)[None, :]
    distance = query_index + window - key_index
    block_start = first_position + jnp.arange(blocks, dtype=jnp.int32)[:, None, None] * window
    allowed = (distance >= 0) & (distance < window) & (block_start - window + key_index >= 0)
    scores = jnp.where(allowed[:, None, None, :, :], scores, -jnp.inf)
    sink_grid = sink_logits.astype(jnp.float32).reshape(kv_count, group_size)[None, :, :, None, None]
    row_peak = jnp.maximum(lax.optimization_barrier(jnp.max(scores, axis=-1, keepdims=True)), sink_grid)
    shifted_exp = jnp.exp(scores - row_peak)
    denominator = lax.optimization_barrier(jnp.sum(shifted_exp, axis=-1, keepdims=True)) + jnp.exp(sink_grid - row_peak)
    probs = (shifted_exp / denominator).astype(jnp.bfloat16)
    attended = jnp.einsum('nhgqk,nkhd->nqhgd', probs.astype(jnp.float32), band_values.astype(jnp.float32))
    return attended.astype(jnp.bfloat16).reshape(total_rows, kv_count * group_size * head_size)

def reference(mixer_input, expert_input, gain_mixer, gain_expert, query_weight, key_weight, value_weight, sink_logits, output_weight, expert_choice, route_weights, expert_gate, expert_up, expert_down, shared_gate, shared_up, shared_down):
    head_block = HEADS * HEAD_DIM // N_TP

    def one_sequence(seq_rows):
        normed = rms_scale(seq_rows, gain_mixer)
        queries = jnp.dot(normed, query_weight, preferred_element_type=jnp.float32).astype(jnp.bfloat16)
        key_rows = jnp.dot(normed, key_weight, preferred_element_type=jnp.float32).astype(jnp.bfloat16)
        value_rows = jnp.dot(normed, value_weight, preferred_element_type=jnp.float32).astype(jnp.bfloat16)
        positions = jnp.arange(SEQ_LEN, dtype=jnp.float32)
        angles = positions[:, None] * frequencies(HEAD_DIM)[None, :]
        rot_queries = rotate(queries.reshape(SEQ_LEN, HEADS, HEAD_DIM), angles)
        rot_keys = rotate(key_rows.reshape(SEQ_LEN, KV_HEADS, HEAD_DIM), angles)
        value_heads = value_rows.reshape(SEQ_LEN, KV_HEADS, HEAD_DIM)
        empty_rows = jnp.zeros((WINDOW, KV_HEADS, HEAD_DIM), jnp.bfloat16)
        attended = attend(rot_queries, rot_keys, value_heads, empty_rows, empty_rows, 0, sink_logits)
        mixed_sum = jnp.zeros((SEQ_LEN, D), jnp.float32)
        for slice_index in range(N_TP):
            low_edge = slice_index * head_block
            mixed_sum = mixed_sum + rounded(jnp.dot(attended[:, low_edge:low_edge + head_block], output_weight[low_edge:low_edge + head_block], preferred_element_type=jnp.float32))
        return mixed_sum.astype(jnp.bfloat16)
    mixer_output = lax.map(one_sequence, mixer_input.reshape(SEQS, SEQ_LEN, D)).reshape(TOKENS_A, D)
    normed_rows = rms_scale(expert_input, gain_expert)
    padded_rows = jnp.concatenate([normed_rows, jnp.zeros((1, D), jnp.bfloat16)], axis=0)
    block_count = TOKENS_B // TOK_B_DEV
    assigned = TOK_B_DEV * TOP
    picked_experts = expert_choice.reshape(block_count, assigned)
    onehot = (picked_experts[:, :, None] == jnp.arange(EXPERTS, dtype=jnp.int32)[None, None, :]).astype(jnp.int32)
    slot_ranks = lax.optimization_barrier(jnp.sum(jnp.cumsum(onehot, axis=1) * onehot, axis=-1)) - 1
    block_ids = jnp.arange(block_count, dtype=jnp.int32)[:, None]
    slot_index = (picked_experts * block_count + block_ids) * CAP + slot_ranks
    token_owner = block_ids * TOK_B_DEV + jnp.arange(assigned, dtype=jnp.int32)[None, :] // TOP
    slot_table = jnp.full((EXPERTS * block_count * CAP,), TOKENS_B, jnp.int32).at[slot_index.reshape(-1)].set(token_owner.reshape(-1).astype(jnp.int32))
    weight_table = jnp.zeros((EXPERTS * block_count * CAP,), jnp.float32).at[slot_index.reshape(-1)].set(route_weights.reshape(-1).astype(jnp.float32))
    ff_block = EXPERT_FF // N_TP

    def one_expert(carry, inputs):
        index_row, weight_row, gate_matrix, up_matrix, down_matrix = inputs
        chosen_rows = padded_rows[index_row]
        gate_values = jnp.dot(chosen_rows, gate_matrix, preferred_element_type=jnp.float32)
        up_values = jnp.dot(chosen_rows, up_matrix, preferred_element_type=jnp.float32)
        hidden = (jax.nn.silu(gate_values) * up_values).astype(jnp.bfloat16)
        result = jnp.zeros((chosen_rows.shape[0], D), jnp.float32)
        for slice_index in range(N_TP):
            low_edge = slice_index * ff_block
            result = result + rounded(jnp.dot(hidden[:, low_edge:low_edge + ff_block], down_matrix[low_edge:low_edge + ff_block], preferred_element_type=jnp.float32))
        return (carry.at[index_row].add(result * weight_row[:, None]), None)
    routed, unused = lax.scan(one_expert, jnp.zeros((TOKENS_B + 1, D), jnp.float32), (slot_table.reshape(EXPERTS, block_count * CAP), weight_table.reshape(EXPERTS, block_count * CAP), expert_gate, expert_up, expert_down))
    shared_gate_values = jnp.dot(normed_rows, shared_gate, preferred_element_type=jnp.float32)
    shared_up_values = jnp.dot(normed_rows, shared_up, preferred_element_type=jnp.float32)
    shared_hidden = (jax.nn.silu(shared_gate_values) * shared_up_values).astype(jnp.bfloat16)
    shared_block = SHARED_FF // N_TP
    shared_result = jnp.zeros((TOKENS_B, D), jnp.float32)
    for slice_index in range(N_TP):
        low_edge = slice_index * shared_block
        shared_result = shared_result + rounded(jnp.dot(shared_hidden[:, low_edge:low_edge + shared_block], shared_down[low_edge:low_edge + shared_block], preferred_element_type=jnp.float32))
    expert_output = (routed[:TOKENS_B] + shared_result).astype(jnp.bfloat16)
    return (mixer_output, expert_output)
```

```python
import math

import jax
import jax.numpy as jnp
from jax import lax
from jax.sharding import PartitionSpec as P

HEAD_DIM = 64
WINDOW = 128
SEQS = 1
RETURN_CHUNKS = 1


norm_eps = 1e-06
rope_base = 500000.0


def from_behind(value, axis, steps):
    count = lax.axis_size(axis)
    first, last = (max(0, -steps), min(count, count - steps))
    return lax.ppermute(value, axis, [(source, source + steps) for source in range(first, last)])


def shifted(value, steps):
    count = lax.axis_size("tp")
    return lax.ppermute(value, "tp", [(source, (source + steps) % count) for source in range(count)])


def rms_scale(matrix, scaling):
    widened = matrix.astype(jnp.float32)
    scaled = widened * lax.rsqrt(jnp.mean(widened * widened, axis=-1, keepdims=True) + norm_eps)
    return (scaled * scaling).astype(jnp.bfloat16)


def frequencies(head_size):
    half_steps = jnp.arange(head_size // 2, dtype=jnp.float32)
    return rope_base ** (-(2.0 * half_steps) / head_size)


def rotate(heads, angles):
    middle = heads.shape[-1] // 2
    widened = heads.astype(jnp.float32)
    cosine = jnp.cos(angles)[:, None, :]
    sine_val = jnp.sin(angles)[:, None, :]
    leading = widened[..., :middle]
    trailing = widened[..., middle:]
    turned = jnp.concatenate(
        [leading * cosine - trailing * sine_val, trailing * cosine + leading * sine_val], axis=-1
    )
    return turned.astype(jnp.bfloat16)


def attend(
    query_heads, key_heads, value_heads, prior_keys, prior_values, first_position, sink_logits
):
    window = prior_keys.shape[0]
    total_rows, kv_count, head_size = key_heads.shape
    group_size = query_heads.shape[1] // kv_count
    blocks = total_rows // window

    def banded(earlier, current):
        joined = jnp.concatenate([earlier, current], axis=0).reshape(
            blocks + 1, window, kv_count, head_size
        )
        return jnp.concatenate([joined[:-1], joined[1:]], axis=1)

    band_keys = banded(prior_keys, key_heads)
    band_values = banded(prior_values, value_heads)
    query_blocks = query_heads.reshape(blocks, window, kv_count, group_size, head_size)
    scores = jnp.einsum(
        "nqhgd,nkhd->nhgqk", query_blocks, band_keys, preferred_element_type=jnp.float32
    ) / math.sqrt(head_size)
    query_index = jnp.arange(window, dtype=jnp.int32)[:, None]
    key_index = jnp.arange(2 * window, dtype=jnp.int32)[None, :]
    distance = query_index + window - key_index
    block_start = first_position + jnp.arange(blocks, dtype=jnp.int32)[:, None, None] * window
    allowed = (distance >= 0) & (distance < window) & (block_start - window + key_index >= 0)
    scores = jnp.where(allowed[:, None, None, :, :], scores, -jnp.inf)
    sink_grid = sink_logits.reshape(kv_count, group_size)[None, :, :, None, None]
    row_peak = jnp.maximum(jnp.max(scores, axis=-1, keepdims=True), sink_grid)
    shifted_exp = jnp.exp(scores - row_peak)
    denominator = jnp.sum(shifted_exp, axis=-1, keepdims=True) + jnp.exp(sink_grid - row_peak)
    probs = (shifted_exp / denominator).astype(jnp.bfloat16)
    attended = jnp.einsum(
        "nhgqk,nkhd->nqhgd", probs, band_values, preferred_element_type=jnp.float32
    )
    return attended.astype(jnp.bfloat16).reshape(total_rows, kv_count * group_size * head_size)


def local(
    mixer_input,
    expert_input,
    gain_mixer,
    gain_expert,
    query_weight,
    key_weight,
    value_weight,
    sink_logits,
    output_weight,
    expert_choice,
    route_weights,
    expert_gate,
    expert_up,
    expert_down,
    shared_gate,
    shared_up,
    shared_down,
):
    tp_count = lax.axis_size("tp")
    ep_count = lax.axis_size("ep")
    tp_rank = lax.axis_index("tp")
    group_rows, model_width = mixer_input.shape

    gate, up, down = expert_gate[0], expert_up[0], expert_down[0]
    half = down.shape[0] // 2
    gate_left, up_left, down_left = (shifted(w, 1) for w in (gate, up, down))
    gate_right, up_right, down_right = (shifted(w, -1) for w in (gate, up, down))
    gate_far = shifted(gate_left, 1)
    up_far = shifted(up_right, -1)
    down_far_low = shifted(down_left[:half], 1)
    down_far_high = shifted(down_right[half:], -1)

    own_tokens = expert_input.shape[0] // tp_count
    top_count = expert_choice.shape[1]
    experts_all = expert_gate.shape[0] * ep_count
    capacity = 2 * own_tokens * top_count // experts_all
    slots = experts_all * capacity
    own_choice = lax.dynamic_slice_in_dim(expert_choice, tp_rank * own_tokens, own_tokens, 0)
    own_weights = lax.dynamic_slice_in_dim(route_weights, tp_rank * own_tokens, own_tokens, 0)
    flat = own_choice.T.reshape(-1)
    assigned = flat.shape[0]
    same = flat[:, None] == flat[None, :]
    order = jnp.arange(assigned, dtype=jnp.int32)
    ranks = jnp.sum((same & (order[None, :] < order[:, None])).astype(jnp.int32), axis=1)
    slot = (flat * capacity + ranks).reshape(top_count, own_tokens)
    hits = slot[:, :, None] == jnp.arange(slots, dtype=jnp.int32)[None, None, :]
    picks = jnp.any(hits, axis=0).astype(jnp.bfloat16)
    shares = jnp.sum(jnp.where(hits, own_weights.T[:, :, None], 0.0), axis=0)

    normed_rows = rms_scale(expert_input, gain_expert)
    own_rows = lax.dynamic_slice_in_dim(normed_rows, tp_rank * own_tokens, own_tokens, 0)
    outgoing = lax.dot_general(
        picks, own_rows, (((0,), (0,)), ((), ())), preferred_element_type=jnp.float32
    ).astype(jnp.bfloat16)
    arrived = lax.all_to_all(
        outgoing.reshape(experts_all, capacity, model_width), "ep", 0, 0, tiled=True
    ).reshape(slots, model_width)

    normed = rms_scale(mixer_input, gain_mixer)
    queries = jnp.dot(normed, query_weight, preferred_element_type=jnp.float32).astype(jnp.bfloat16)
    key_rows = jnp.dot(normed, key_weight, preferred_element_type=jnp.float32).astype(jnp.bfloat16)
    value_rows = jnp.dot(normed, value_weight, preferred_element_type=jnp.float32).astype(
        jnp.bfloat16
    )
    first_position = lax.axis_index("ep") % (ep_count // SEQS) * group_rows
    positions = (first_position + jnp.arange(group_rows, dtype=jnp.int32)).astype(jnp.float32)
    angles = positions[:, None] * frequencies(HEAD_DIM)[None, :]
    rot_queries = rotate(queries.reshape(group_rows, -1, HEAD_DIM), angles)
    rot_keys = rotate(key_rows.reshape(group_rows, -1, HEAD_DIM), angles)
    key_width = key_rows.shape[1]
    tail_start = group_rows - WINDOW
    tail_pair = jnp.concatenate(
        [rot_keys.reshape(group_rows, key_width)[tail_start:], value_rows[tail_start:]], axis=1
    )
    earlier_pair = from_behind(tail_pair, "ep", 1)
    prior_keys = earlier_pair[:, :key_width].reshape(WINDOW, -1, HEAD_DIM)
    prior_values = earlier_pair[:, key_width:].reshape(WINDOW, -1, HEAD_DIM)
    attended = attend(
        rot_queries,
        rot_keys,
        value_rows.reshape(group_rows, -1, HEAD_DIM),
        prior_keys,
        prior_values,
        first_position,
        sink_logits,
    )
    mixed = jnp.dot(attended, output_weight, preferred_element_type=jnp.float32).astype(jnp.bfloat16)

    gate_values = jnp.dot(normed_rows, shared_gate, preferred_element_type=jnp.float32)
    up_values = jnp.dot(normed_rows, shared_up, preferred_element_type=jnp.float32)
    hidden = (jax.nn.silu(gate_values) * up_values).astype(jnp.bfloat16)
    shared = jnp.dot(hidden, shared_down, preferred_element_type=jnp.float32).astype(jnp.bfloat16)

    def hidden_of(gate_part, up_part):
        gate_values = jnp.dot(arrived, gate_part, preferred_element_type=jnp.float32)
        up_values = jnp.dot(arrived, up_part, preferred_element_type=jnp.float32)
        return (jax.nn.silu(gate_values) * up_values).astype(jnp.bfloat16)

    hidden_own = hidden_of(gate, up)
    hidden_left = hidden_of(gate_left, up_left)
    hidden_right = hidden_of(gate_right, up_right)
    hidden_far = hidden_of(gate_far, up_far)
    terms = (
        (hidden_own, down),
        (hidden_left, down_left),
        (hidden_right, down_right),
        (hidden_far[:, :half], down_far_low),
        (hidden_far[:, half:], down_far_high),
    )
    width = model_width // RETURN_CHUNKS
    returned = []
    for chunk in range(RETURN_CHUNKS):
        cut = slice(chunk * width, (chunk + 1) * width)
        result = sum(
            jnp.dot(units, part[:, cut], preferred_element_type=jnp.float32) for units, part in terms
        )
        returned.append(
            lax.all_to_all(
                result.astype(jnp.bfloat16).reshape(experts_all, capacity, width), "ep", 0, 0, tiled=True
            ).reshape(slots, width)
        )

    def piece(rows, steps):
        owner = (tp_rank + steps) % tp_count
        return lax.dynamic_slice_in_dim(rows, owner * own_tokens, own_tokens, 0)

    def plus(*parts):
        return sum(part.astype(jnp.float32) for part in parts)

    mixed_far = shifted(piece(mixed, 2), 1)
    shared_far = shifted(piece(shared, 2), -1)
    mixed_left = shifted(plus(piece(mixed, 1), mixed_far).astype(jnp.bfloat16), 1)
    mixed_right = shifted(piece(mixed, -1), -1)
    shared_left = shifted(piece(shared, 1), 1)
    shared_right = shifted(plus(piece(shared, -1), shared_far).astype(jnp.bfloat16), -1)
    mixer_output = plus(piece(mixed, 0), mixed_left, mixed_right).astype(jnp.bfloat16)
    shared_part = plus(piece(shared, 0), shared_left, shared_right)

    coarse = shares.astype(jnp.bfloat16)
    fine = (shares - coarse.astype(jnp.float32)).astype(jnp.bfloat16)
    weights = jnp.concatenate([coarse, fine], axis=0)
    routed = []
    for rows in returned:
        both = jnp.dot(weights, rows, preferred_element_type=jnp.float32)
        routed.append(both[:own_tokens] + both[own_tokens:])
    expert_output = (jnp.concatenate(routed, axis=1) + shared_part).astype(jnp.bfloat16)
    return (mixer_output, expert_output)


def solution(mesh):
    placed = (
        P("ep", None),
        P("ep", None),
        P(),
        P(),
        P(None, "tp"),
        P(None, "tp"),
        P(None, "tp"),
        P("tp"),
        P("tp", None),
        P("ep", None),
        P("ep", None),
        P("ep", None, "tp"),
        P("ep", None, "tp"),
        P("ep", "tp", None),
        P(None, "tp"),
        P(None, "tp"),
        P("tp", None),
    )
    return jax.shard_map(
        local,
        mesh=mesh,
        in_specs=placed,
        out_specs=(P(("ep", "tp"), None), P(("ep", "tp"), None)),
        check_vma=False,
    )
```

```python
import functools
import math

import jax
import jax.numpy as jnp
from jax import lax
from jax.experimental import pallas as pl
from jax.experimental.pallas import tpu as pltpu
from jax.sharding import PartitionSpec as P

HEAD_DIM = 64
WINDOW = 128
MESH = pl.DeviceIdType.MESH

norm_eps = 1e-06
rope_base = 500000.0

GROUP = 512
OWN = 128
WIDTH = 2048
EP = 64
CAP = 8
SLOTS = EP * CAP
PART = 256
SHARED = 128
CHUNKS = 4
COLS = WIDTH // CHUNKS
PAIRS = 3
TP = 4

GATE_L, UP_L, GATE_R, UP_R, GATE_F, UP_F = range(6)
DOWN_L, DOWN_R, DOWN_FL, DOWN_FR = 6, 10, 14, 18
MIX_F, SH_F, MIX_L, SH_L, MIX_R, SH_R, TAIL = range(22, 29)
MESSAGES = 29

f32, bf16 = jnp.float32, jnp.bfloat16


def dot(a, b):
    return jnp.dot(a, b, preferred_element_type=f32)


def kernel(
    xa, xb, wq, wkv, wo, sgate, sup, sdown, gate_in, up_in, down_in,
    gain_a, gain_b, sinks, choice_rows, choice_cols, route, cosine, sine,
    mixer_out, expert_out,
    xa_v, xb_v, na, nb, wq_v, wkv_v, wo_v, sg_v, su_v, sd_v,
    gate, up, down, out, arr, rows, hid, res, ret,
    qs, kvx, att, sh_hid, mix, sh, mix_got, sh_got, routed, weights, picks,
    load_sem, send_sem, recv_sem, x_send, x_recv,
):
    me = lax.axis_index("ep")
    t = lax.axis_index("tp")
    right = lax.rem(t + 1, TP)
    left = lax.rem(t + TP - 1, TP)
    far = lax.rem(t + 2, TP)

    barrier = pltpu.get_barrier_semaphore()

    def greet(s, _):
        pl.semaphore_signal(barrier, inc=1, device_id={"ep": lax.rem(me + s, EP)}, device_id_type=MESH)
        return _

    for neighbour in (left, right):
        pl.semaphore_signal(barrier, inc=1, device_id={"tp": neighbour}, device_id_type=MESH)
    lax.fori_loop(1, EP, greet, 0)

    loads = {}

    def load(name, src, dst):
        copy = pltpu.make_async_copy(src, dst, load_sem.at[len(loads)])
        copy.start()
        loads[name] = copy

    load("xb", xb, xb_v)
    load("sg", sgate, sg_v)
    load("su", sup, su_v)
    load("sd", sdown, sd_v)
    load("xa", xa, xa_v)
    load("wq", wq, wq_v)
    load("wkv", wkv, wkv_v)
    load("wo", wo, wo_v)
    load("gate", gate_in, gate.at[0])
    load("up", up_in, up.at[0])
    for c in range(CHUNKS):
        load(f"down{c}", down_in.at[:, pl.ds(c * COLS, COLS)], down.at[c, pl.ds(0, PART)])

    messages = {}

    def message(number, src, dst, to):
        copy = pltpu.make_async_remote_copy(
            src_ref=src, dst_ref=dst, send_sem=send_sem.at[number], recv_sem=recv_sem.at[number],
            device_id=to, device_id_type=MESH,
        )
        copy.start()
        messages[number] = copy

    own = pl.ds(pl.multiple_of(t * OWN, OWN), OWN)
    row_a = choice_rows[0:1, own].astype(f32)
    row_b = choice_rows[1:2, own].astype(f32)
    cols = choice_cols[own, :].astype(f32)
    col_a, col_b = cols[:, 0:1], cols[:, 1:2]
    down_i = lax.broadcasted_iota(jnp.int32, (OWN, OWN), 0)
    across_i = lax.broadcasted_iota(jnp.int32, (OWN, OWN), 1)

    def count(condition, axis):
        return jnp.sum(jnp.where(condition, 1.0, 0.0).astype(f32), axis=axis, keepdims=True)

    before = down_i < across_i
    after = down_i > across_i
    slot_row_a = row_a * CAP + count((col_a == row_a) & before, 0)
    slot_row_b = row_b * CAP + count(col_a == row_b, 0) + count((col_b == row_b) & before, 0)
    slot_col_a = col_a * CAP + count((col_a == row_a) & after, 1)
    slot_col_b = col_b * CAP + count(col_b == row_a, 1) + count((col_b == row_b) & after, 1)
    slot_i = lax.broadcasted_iota(jnp.int32, (SLOTS, OWN), 0).astype(f32)
    picks[...] = jnp.where((slot_i == slot_row_a) | (slot_i == slot_row_b), 1.0, 0.0).astype(bf16)
    slot_j = lax.broadcasted_iota(jnp.int32, (OWN, SLOTS), 1).astype(f32)
    shares = route[own, :]
    share = jnp.where(slot_j == slot_col_a, shares[:, 0:1], 0.0) + jnp.where(
        slot_j == slot_col_b, shares[:, 1:2], 0.0
    )
    coarse = share.astype(bf16)
    weights[0:OWN, :] = coarse
    weights[OWN:, :] = (share - coarse.astype(f32)).astype(bf16)

    def normalise(src, dst, gain, start, count_of):
        step = 32

        def body(i, _):
            at = pl.ds(pl.multiple_of(start + i * step, step), step)
            wide = src[at, :].astype(f32)
            scale = lax.rsqrt(jnp.mean(wide * wide, axis=-1, keepdims=True) + norm_eps)
            dst[at, :] = (wide * scale * gain[...]).astype(bf16)
            return _

        lax.fori_loop(0, count_of // step, body, 0)

    loads["xb"].wait()
    normalise(xb_v, nb, gain_b, t * OWN, OWN)

    pl.semaphore_wait(barrier, EP + 1)

    message(GATE_L, gate_in, gate.at[1], {"tp": right})
    message(GATE_R, gate_in, gate.at[2], {"tp": left})
    message(UP_L, up_in, up.at[1], {"tp": right})
    message(UP_R, up_in, up.at[2], {"tp": left})

    def gather(c, _):
        at = pl.ds(pl.multiple_of(c * COLS, COLS), COLS)
        got = dot(picks[...], nb[own, at])
        out[:, :, at] = got.reshape(EP, CAP, COLS).astype(bf16)
        return _

    lax.fori_loop(0, CHUNKS, gather, 0)

    def exchange(src_of, dst, number):
        def body(s, _):
            peer = lax.rem(me + s, EP)
            pltpu.make_async_remote_copy(
                src_ref=src_of(peer), dst_ref=dst, send_sem=x_send.at[number], recv_sem=x_recv.at[number],
                device_id={"ep": peer}, device_id_type=MESH,
            ).start()
            return _

        lax.fori_loop(1, EP, body, 0)

    def all_blocks(src, dst, number):
        most = pl.ds(0, EP - 1)
        return pltpu.make_async_remote_copy(
            src_ref=src.at[most], dst_ref=dst.at[most], send_sem=x_send.at[number], recv_sem=x_recv.at[number],
            device_id={"ep": lax.rem(me + 1, EP)}, device_id_type=MESH,
        )

    exchange(lambda peer: out.at[peer], arr.at[me], 0)
    arr[me] = out[me]

    normalise(xb_v, nb, gain_b, 0, GROUP)
    for name in ("sg", "su", "sd"):
        loads[name].wait()

    def shared(i, _):
        at = pl.ds(pl.multiple_of(i * OWN, OWN), OWN)
        g = dot(nb[at, :], sg_v[...])
        u = dot(nb[at, :], su_v[...])
        units = (g / (1.0 + jnp.exp(-g)) * u).astype(bf16)
        for c in range(CHUNKS):
            part = pl.ds(c * COLS, COLS)
            sh[at, part] = dot(units, sd_v[:, part]).astype(bf16)
        return _

    lax.fori_loop(0, TP, shared, 0)

    for name in ("xa", "wq", "wkv"):
        loads[name].wait()
    normalise(xa_v, na, gain_a, 0, GROUP)
    lane = lax.broadcasted_iota(jnp.int32, (OWN, 128), 1)
    first_half = (lane & 63) < 32
    is_key = lane < 64

    def turn(value, c, s):
        value = value.astype(bf16).astype(f32)
        partner = jnp.where(first_half, pltpu.roll(value, 96, 1), pltpu.roll(value, 32, 1))
        return (value * c + partner * s).astype(bf16)

    def project(i, _):
        at = pl.ds(pl.multiple_of(i * OWN, OWN), OWN)
        c, s = cosine[at, :], sine[at, :]
        q = dot(na[at, :], wq_v[...])
        for p in range(PAIRS):
            qs[i, p * OWN : (p + 1) * OWN, :] = turn(q[:, p * 128 : (p + 1) * 128], c, s)
        kv = dot(na[at, :], wkv_v[...])
        after_tail = pl.ds(pl.multiple_of(WINDOW + i * OWN, OWN), OWN)
        kvx[after_tail, :] = turn(kv, jnp.where(is_key, c, 1.0), jnp.where(is_key, s, 0.0))
        return _

    lax.fori_loop(0, TP, project, 0)
    message(TAIL, kvx.at[pl.ds(GROUP, WINDOW)], kvx.at[pl.ds(0, WINDOW)], {"ep": lax.rem(me + 1, EP)})
    messages[TAIL].wait_recv()

    band_lane = lax.broadcasted_iota(jnp.int32, (2 * WINDOW, 128), 1)
    band_key = band_lane < 64
    query_i = lax.broadcasted_iota(jnp.int32, (PAIRS * OWN, 2 * WINDOW), 0) & (WINDOW - 1)
    key_i = lax.broadcasted_iota(jnp.int32, (PAIRS * OWN, 2 * WINDOW), 1)
    distance = query_i + WINDOW - key_i
    in_window = (distance >= 0) & (distance < WINDOW)
    head_row = lax.broadcasted_iota(jnp.int32, (PAIRS * OWN, 1), 0)
    sink_of = [
        jnp.where(
            head_row < OWN, sinks[odd], jnp.where(head_row < 2 * OWN, sinks[2 + odd], sinks[4 + odd])
        )
        for odd in (0, 1)
    ]

    def attend(n, _):
        band = kvx[pl.ds(pl.multiple_of(n * OWN, OWN), 2 * WINDOW), :].astype(f32)
        keys = jnp.where(band_key, band, 0.0)
        values = jnp.where(band_key, 0.0, band)
        key_sets = (keys.astype(bf16), pltpu.roll(keys, 64, 1).astype(bf16))
        value_sets = (pltpu.roll(values, 64, 1).astype(bf16), values.astype(bf16))
        allowed = in_window & (me * GROUP + n * OWN - WINDOW + key_i >= 0)
        q = qs[n]
        total = jnp.zeros((PAIRS * OWN, 128), f32)
        for odd in (0, 1):
            scores = lax.dot_general(
                q, key_sets[odd], (((1,), (1,)), ((), ())), preferred_element_type=f32
            ) * (1.0 / math.sqrt(HEAD_DIM))
            scores = jnp.where(allowed, scores, -jnp.inf)
            peak = jnp.maximum(jnp.max(scores, axis=-1, keepdims=True), sink_of[odd])
            e = jnp.exp(scores - peak)
            denominator = jnp.sum(e, axis=-1, keepdims=True) + jnp.exp(sink_of[odd] - peak)
            total = total + dot((e / denominator).astype(bf16), value_sets[odd])
        at = pl.ds(pl.multiple_of(n * OWN, OWN), OWN)
        for p in range(PAIRS):
            att[at, p * 128 : (p + 1) * 128] = total[p * OWN : (p + 1) * OWN].astype(bf16)
        return _

    lax.fori_loop(0, TP, attend, 0)

    messages[GATE_L].wait_recv()
    message(GATE_F, gate.at[1], gate.at[3], {"tp": right})
    messages[UP_R].wait_recv()
    message(UP_F, up.at[2], up.at[3], {"tp": left})

    def send_down(c):
        src = down_in.at[:, pl.ds(c * COLS, COLS)]
        message(DOWN_L + c, src, down.at[c, pl.ds(PART, PART)], {"tp": right})
        message(DOWN_R + c, src, down.at[c, pl.ds(2 * PART, PART)], {"tp": left})

    send_down(0)
    send_down(1)

    loads["wo"].wait()

    def project_out(i, _):
        at = pl.ds(pl.multiple_of(i * OWN, OWN), OWN)
        for c in range(CHUNKS):
            part = pl.ds(c * COLS, COLS)
            mix[at, part] = dot(att[at, :], wo_v[:, part]).astype(bf16)
        return _

    lax.fori_loop(0, TP, project_out, 0)

    all_blocks(out, arr, 0).wait_recv()

    def flatten(c, _):
        at = pl.ds(pl.multiple_of(c * COLS, COLS), COLS)
        rows[:, at] = arr[:, :, at].astype(f32).reshape(SLOTS, COLS).astype(bf16)
        return _

    lax.fori_loop(0, CHUNKS, flatten, 0)

    def hidden(q):
        def body(i, _):
            at = pl.ds(pl.multiple_of(i * 256, 256), 256)
            g = dot(rows[at, :], gate[q])
            u = dot(rows[at, :], up[q])
            hid[at, q * PART : (q + 1) * PART] = (g / (1.0 + jnp.exp(-g)) * u).astype(bf16)
            return _

        lax.fori_loop(0, SLOTS // 256, body, 0)

    loads["gate"].wait()
    loads["up"].wait()
    hidden(0)
    messages[UP_L].wait_recv()
    hidden(1)
    messages[GATE_R].wait_recv()
    hidden(2)
    messages[GATE_F].wait_recv()
    messages[UP_F].wait_recv()
    hidden(3)

    half = PART // 2

    def finish(c):
        loads[f"down{c}"].wait()
        messages[DOWN_FL + c].wait_recv()
        messages[DOWN_FR + c].wait_recv()

        def body(i, _):
            at = pl.ds(pl.multiple_of(i * 256, 256), 256)
            got = dot(hid[at, :], down[c])
            blocks = pl.ds(i * (256 // CAP), 256 // CAP)
            res[c, blocks] = got.reshape(256 // CAP, CAP, COLS).astype(bf16)
            return _

        lax.fori_loop(0, SLOTS // 256, body, 0)
        exchange(lambda peer: res.at[c, peer], ret.at[c, me], 1 + c)
        ret[c, me] = res[c, me]

    for c in range(CHUNKS):
        messages[DOWN_L + c].wait_recv()
        message(
            DOWN_FL + c, down.at[c, pl.ds(PART, half)], down.at[c, pl.ds(3 * PART, half)], {"tp": right}
        )
        messages[DOWN_R + c].wait_recv()
        message(
            DOWN_FR + c, down.at[c, pl.ds(2 * PART + half, half)], down.at[c, pl.ds(3 * PART + half, half)],
            {"tp": left},
        )
        if c + 2 < CHUNKS:
            send_down(c + 2)
        else:
            if c + 2 == CHUNKS:
                pass
        if c >= 1:
            finish(c - 1)

    def piece(ref, owner):
        return ref.at[pl.ds(pl.multiple_of(owner * OWN, OWN), OWN)]

    message(MIX_F, piece(mix, far), mix_got.at[0], {"tp": right})
    message(SH_F, piece(sh, far), sh_got.at[0], {"tp": left})
    message(SH_L, piece(sh, right), sh_got.at[1], {"tp": right})
    message(MIX_R, piece(mix, left), mix_got.at[2], {"tp": left})
    finish(CHUNKS - 1)

    def combine(c):
        all_blocks(res.at[c], ret.at[c], 1 + c).wait_recv()
        got = ret[c].astype(f32).reshape(SLOTS, COLS).astype(bf16)
        both = dot(weights[...], got)
        routed[:, c * COLS : (c + 1) * COLS] = both[0:OWN] + both[OWN:]

    def add_into(ref, owner, extra):
        at = pl.ds(pl.multiple_of(owner * OWN, OWN), OWN)
        ref[at, :] = (ref[at, :].astype(f32) + extra[...].astype(f32)).astype(bf16)

    combine(0)
    messages[MIX_F].wait_recv()
    add_into(mix, right, mix_got.at[0])
    message(MIX_L, piece(mix, right), mix_got.at[1], {"tp": right})
    messages[SH_F].wait_recv()
    add_into(sh, left, sh_got.at[0])
    message(SH_R, piece(sh, left), sh_got.at[2], {"tp": left})
    for c in range(1, CHUNKS):
        combine(c)

    messages[MIX_R].wait_recv()
    messages[MIX_L].wait_recv()
    mixer_out[...] = (
        mix[own, :].astype(f32) + mix_got[1].astype(f32) + mix_got[2].astype(f32)
    ).astype(bf16)
    messages[SH_L].wait_recv()
    messages[SH_R].wait_recv()
    expert_out[...] = (
        routed[...] + sh[own, :].astype(f32) + sh_got[1].astype(f32) + sh_got[2].astype(f32)
    ).astype(bf16)

    for copy in messages.values():
        copy.wait_send()
    all_blocks(out, arr, 0).wait_send()
    for c in range(CHUNKS):
        all_blocks(res.at[c], ret.at[c], 1 + c).wait_send()


def local(
    mixer_input, expert_input, gain_mixer, gain_expert, query_weight, key_weight, value_weight,
    sink_logits, output_weight, expert_choice, route_weights, expert_gate, expert_up, expert_down,
    shared_gate, shared_up, shared_down,
):
    half_steps = jnp.arange(HEAD_DIM // 2, dtype=f32)
    steps = rope_base ** (-(2.0 * half_steps) / HEAD_DIM)
    positions = (lax.axis_index("ep") * GROUP + jnp.arange(GROUP, dtype=jnp.int32)).astype(f32)
    angles = positions[:, None] * steps[None, :]
    cosine, sine = jnp.cos(angles), jnp.sin(angles)
    cosine = jnp.concatenate([cosine] * 4, axis=1)
    sine = jnp.concatenate([-sine, sine, -sine, sine], axis=1)
    key_value = jnp.concatenate([key_weight, value_weight], axis=1)

    anywhere = pl.BlockSpec(memory_space=pl.ANY)
    vmem = pl.BlockSpec(memory_space=pltpu.VMEM)
    smem = pl.BlockSpec(memory_space=pltpu.SMEM)
    V = pltpu.VMEM
    scratch = [
        V((GROUP, WIDTH), bf16), V((GROUP, WIDTH), bf16), V((GROUP, WIDTH), bf16), V((GROUP, WIDTH), bf16),
        V((WIDTH, 384), bf16), V((WIDTH, 128), bf16), V((384, WIDTH), bf16),
        V((WIDTH, SHARED), bf16), V((WIDTH, SHARED), bf16), V((SHARED, WIDTH), bf16),
        V((TP, WIDTH, PART), bf16), V((TP, WIDTH, PART), bf16), V((CHUNKS, TP * PART, COLS), bf16),
        V((EP, CAP, WIDTH), bf16), V((EP, CAP, WIDTH), bf16), V((SLOTS, WIDTH), bf16),
        V((SLOTS, TP * PART), bf16), V((CHUNKS, EP, CAP, COLS), bf16), V((CHUNKS, EP, CAP, COLS), bf16),
        V((TP, PAIRS * OWN, 128), bf16), V((WINDOW + GROUP, 128), bf16), V((GROUP, 384), bf16),
        V((OWN, SHARED), bf16), V((GROUP, WIDTH), bf16), V((GROUP, WIDTH), bf16),
        V((3, OWN, WIDTH), bf16), V((3, OWN, WIDTH), bf16), V((OWN, WIDTH), f32),
        V((2 * OWN, SLOTS), bf16), V((SLOTS, OWN), bf16),
        pltpu.SemaphoreType.DMA((16,)), pltpu.SemaphoreType.DMA((MESSAGES,)),
        pltpu.SemaphoreType.DMA((MESSAGES,)), pltpu.SemaphoreType.DMA((1 + CHUNKS,)),
        pltpu.SemaphoreType.DMA((1 + CHUNKS,)),
    ]
    shape = jax.ShapeDtypeStruct((OWN, WIDTH), bf16)
    return pl.pallas_call(
        kernel,
        out_shape=(shape, shape),
        in_specs=[anywhere] * 11 + [vmem] * 2 + [smem] + [vmem] * 5,
        out_specs=(vmem, vmem),
        scratch_shapes=scratch,
        compiler_params=pltpu.CompilerParams(
            collective_id=0, has_side_effects=True, vmem_limit_bytes=63 * 2**20
        ),
        name="everything",
    )(
        mixer_input, expert_input, query_weight, key_value, output_weight,
        shared_gate, shared_up, shared_down, expert_gate[0], expert_up[0], expert_down[0],
        gain_mixer[None], gain_expert[None], sink_logits, expert_choice.T, expert_choice, route_weights,
        cosine, sine,
    )


def solution(mesh):
    placed = (
        P("ep", None),
        P("ep", None),
        P(),
        P(),
        P(None, "tp"),
        P(None, "tp"),
        P(None, "tp"),
        P("tp"),
        P("tp", None),
        P("ep", None),
        P("ep", None),
        P("ep", None, "tp"),
        P("ep", None, "tp"),
        P("ep", "tp", None),
        P(None, "tp"),
        P(None, "tp"),
        P("tp", None),
    )
    return jax.shard_map(
        local,
        mesh=mesh,
        in_specs=placed,
        out_specs=(P(("ep", "tp"), None), P(("ep", "tp"), None)),
        check_vma=False,
    )
```

```python
import functools
import math

import jax
import jax.numpy as jnp
from jax import lax
from jax.experimental import pallas as pl
from jax.experimental.pallas import tpu as pltpu
from jax.sharding import PartitionSpec as P

HEAD_DIM = 64
WINDOW = 128
MESH = pl.DeviceIdType.MESH

norm_eps = 1e-06
rope_base = 500000.0

GROUP = 512
OWN = 128
WIDTH = 2048
EP = 64
CAP = 8
SLOTS = EP * CAP
PART = 256
SHARED = 128
COLS = 512
CUTS = (128, 128, 128, 128) + (256,) * 6
CHUNKS = len(CUTS)
STARTS = tuple(sum(CUTS[:c]) for c in range(CHUNKS))
ROW = 8
STRIP = SHARED // ROW
HALF = WIDTH // 2
PAIRS = 3
TP = 4

GATE_L, UP_L, GATE_R, UP_R, GATE_F, UP_F, TAIL = range(7)
STRIP_L, STRIP_R, STRIP_FL, STRIP_FR, UNITS_L, UNITS_R, UNITS_F = range(7, 14)
MIX_FL, MIX_FR, MIX_L0, MIX_L1, MIX_R0, MIX_R1 = range(14, 20)
DOWN_L, DOWN_R, DOWN_FL, DOWN_FR = (20 + CHUNKS * k for k in range(4))
MESSAGES = 20 + 4 * CHUNKS

f32, bf16 = jnp.float32, jnp.bfloat16


def dot(a, b):
    return jnp.dot(a, b, preferred_element_type=f32)


def kernel(
    xa, xb, wq, wk, wv, wo, sgate, sup, sdown, gate_in, up_in, down_in,
    gain_a_in, gain_b_in, sinks_in, choice_in, route_in, steps_in,
    mixer_out, expert_out,
    xa_v, xb_v, na, nb, wq_v, wkv_v, wo_v, sg_v, su_v, strips,
    gate, up, out, arr, rows, hid,
    gain_a, gain_b, sinks, choice_rows, route, steps,
    qs, kvx, att, mix, mix_far, mix_got, units, units_got, routed, weights, picks,
    *rest,
):
    down, res, ret = (rest[k * CHUNKS : (k + 1) * CHUNKS] for k in range(3))
    load_sem, send_sem, recv_sem, x_send, x_recv = rest[3 * CHUNKS :]
    me = lax.axis_index("ep")
    t = lax.axis_index("tp")
    right = lax.rem(t + 1, TP)
    left = lax.rem(t + TP - 1, TP)
    far = lax.rem(t + 2, TP)

    barrier = pltpu.get_barrier_semaphore()

    def greet(s, _):
        pl.semaphore_signal(barrier, inc=1, device_id={"ep": lax.rem(me + s, EP)}, device_id_type=MESH)
        return _

    for neighbour in (left, right, far):
        pl.semaphore_signal(barrier, inc=1, device_id={"tp": neighbour}, device_id_type=MESH)
    lax.fori_loop(1, EP, greet, 0)

    loads = {}

    def load(name, src, dst):
        copy = pltpu.make_async_copy(src, dst, load_sem.at[len(loads)])
        copy.start()
        loads[name] = copy

    load("choice", choice_in, choice_rows)
    load("route", route_in, route)
    load("gain_b", gain_b_in, gain_b)
    load("xb", xb, xb_v)
    load("gain_a", gain_a_in, gain_a)
    load("sinks", sinks_in, sinks)
    load("steps", steps_in, steps)
    load("sg", sgate, sg_v)
    load("su", sup, su_v)
    load("sd", sdown, strips.at[0])
    load("xa", xa, xa_v)
    load("wq", wq, wq_v)
    load("wk", wk, wkv_v.at[pl.ds(0, HEAD_DIM)])
    load("wv", wv, wkv_v.at[pl.ds(HEAD_DIM, HEAD_DIM)])
    load("wo", wo, wo_v)
    load("gate", gate_in, gate.at[0])
    load("up", up_in, up.at[0])
    for c in range(CHUNKS):
        load(f"down{c}", down_in.at[:, pl.ds(STARTS[c], CUTS[c])], down[c].at[pl.ds(0, PART)])

    messages = {}

    def message(number, src, dst, to):
        copy = pltpu.make_async_remote_copy(
            src_ref=src, dst_ref=dst, send_sem=send_sem.at[number], recv_sem=recv_sem.at[number],
            device_id=to, device_id_type=MESH,
        )
        copy.start()
        messages[number] = copy

    own = pl.ds(pl.multiple_of(t * OWN, OWN), OWN)
    loads["choice"].wait()
    loads["route"].wait()
    row_a = choice_rows[0:1, own].astype(f32)
    row_b = choice_rows[1:2, own].astype(f32)
    down_i = lax.broadcasted_iota(jnp.int32, (OWN, OWN), 0)
    across_i = lax.broadcasted_iota(jnp.int32, (OWN, OWN), 1)

    def column(row):
        return jnp.sum(jnp.where(down_i == across_i, row, 0.0), axis=1, keepdims=True)

    col_a, col_b = column(row_a), column(row_b)

    def count(condition, axis):
        return jnp.sum(jnp.where(condition, 1.0, 0.0).astype(f32), axis=axis, keepdims=True)

    before = down_i < across_i
    after = down_i > across_i
    slot_row_a = row_a * CAP + count((col_a == row_a) & before, 0)
    slot_row_b = row_b * CAP + count(col_a == row_b, 0) + count((col_b == row_b) & before, 0)
    slot_col_a = col_a * CAP + count((col_a == row_a) & after, 1)
    slot_col_b = col_b * CAP + count(col_b == row_a, 1) + count((col_b == row_b) & after, 1)
    slot_i = lax.broadcasted_iota(jnp.int32, (SLOTS, OWN), 0).astype(f32)
    picks[...] = jnp.where((slot_i == slot_row_a) | (slot_i == slot_row_b), 1.0, 0.0).astype(bf16)
    slot_j = lax.broadcasted_iota(jnp.int32, (OWN, SLOTS), 1).astype(f32)
    share = jnp.where(slot_j == slot_col_a, column(route[0:1, own]), 0.0) + jnp.where(
        slot_j == slot_col_b, column(route[1:2, own]), 0.0
    )
    coarse = share.astype(bf16)
    weights[0:OWN, :] = coarse
    weights[OWN:, :] = (share - coarse.astype(f32)).astype(bf16)

    def normalise(src, dst, gain, start, count_of):
        step = 32

        def body(i, _):
            at = pl.ds(pl.multiple_of(start + i * step, step), step)
            wide = src[at, :].astype(f32)
            scale = lax.rsqrt(jnp.mean(wide * wide, axis=-1, keepdims=True) + norm_eps)
            dst[at, :] = (wide * scale * gain[...]).astype(bf16)
            return _

        lax.fori_loop(0, count_of // step, body, 0)

    loads["gain_b"].wait()
    loads["xb"].wait()
    normalise(xb_v, nb, gain_b, t * OWN, OWN)

    pl.semaphore_wait(barrier, EP + 2)

    place = lax.rem(me, ROW)
    strip = pl.ds(pl.multiple_of(place * STRIP, STRIP), STRIP)
    message(STRIP_L, sdown.at[strip], strips.at[1, strip], {"tp": right})
    message(STRIP_R, sdown.at[strip], strips.at[2, strip], {"tp": left})
    message(GATE_L, gate_in, gate.at[1], {"tp": right})
    message(UP_R, up_in, up.at[2], {"tp": left})
    message(UP_L, up_in, up.at[1], {"tp": right})
    message(GATE_R, gate_in, gate.at[2], {"tp": left})

    def send_down(c):
        src = down_in.at[:, pl.ds(STARTS[c], CUTS[c])]
        message(DOWN_L + c, src, down[c].at[pl.ds(PART, PART)], {"tp": right})
        message(DOWN_R + c, src, down[c].at[pl.ds(2 * PART, PART)], {"tp": left})

    send_down(0)

    def gather(c, _):
        at = pl.ds(pl.multiple_of(c * COLS, COLS), COLS)
        got = dot(picks[...], nb[own, at])
        out[:, :, at] = got.reshape(EP, CAP, COLS).astype(bf16)
        return _

    lax.fori_loop(0, WIDTH // COLS, gather, 0)

    def exchange(src_of, dst, number):
        def body(s, _):
            peer = lax.rem(me + s, EP)
            pltpu.make_async_remote_copy(
                src_ref=src_of(peer), dst_ref=dst, send_sem=x_send.at[number], recv_sem=x_recv.at[number],
                device_id={"ep": peer}, device_id_type=MESH,
            ).start()
            return _

        lax.fori_loop(1, EP, body, 0)

    def all_blocks(src, dst, number):
        most = pl.ds(0, EP - 1)
        return pltpu.make_async_remote_copy(
            src_ref=src.at[most], dst_ref=dst.at[most], send_sem=x_send.at[number], recv_sem=x_recv.at[number],
            device_id={"ep": lax.rem(me + 1, EP)}, device_id_type=MESH,
        )

    exchange(lambda peer: out.at[peer], arr.at[me], 0)
    arr[me] = out[me]

    normalise(xb_v, nb, gain_b, 0, GROUP)
    for name in ("sg", "su", "sd"):
        loads[name].wait()

    def shared(i, _):
        at = pl.ds(pl.multiple_of(i * OWN, OWN), OWN)
        g = dot(nb[at, :], sg_v[...])
        u = dot(nb[at, :], su_v[...])
        units[at, :] = (g / (1.0 + jnp.exp(-g)) * u).astype(bf16)
        return _

    lax.fori_loop(0, TP, shared, 0)

    for name in ("xa", "wq", "wk", "wv", "gain_a", "sinks", "steps"):
        loads[name].wait()
    normalise(xa_v, na, gain_a, 0, GROUP)
    lane = lax.broadcasted_iota(jnp.int32, (OWN, 128), 1)
    first_half = (lane & 63) < 32
    is_key = lane < 64

    def turn(value, c, s):
        value = value.astype(bf16).astype(f32)
        partner = jnp.where(first_half, pltpu.roll(value, 96, 1), pltpu.roll(value, 32, 1))
        return (value * c + partner * s).astype(bf16)

    def project(i, _):
        at = pl.ds(pl.multiple_of(i * OWN, OWN), OWN)
        position = me * GROUP + i * OWN + down_i
        angles = position.astype(f32) * steps[...]
        c, s = jnp.cos(angles), jnp.sin(angles)
        s = jnp.where(first_half, -s, s)
        q = dot(na[at, :], wq_v[...])
        for p in range(PAIRS):
            qs[i, p * OWN : (p + 1) * OWN, :] = turn(q[:, p * 128 : (p + 1) * 128], c, s)
        kv = lax.dot_general(na[at, :], wkv_v[...], (((1,), (1,)), ((), ())), preferred_element_type=f32)
        after_tail = pl.ds(pl.multiple_of(WINDOW + i * OWN, OWN), OWN)
        kvx[after_tail, :] = turn(kv, jnp.where(is_key, c, 1.0), jnp.where(is_key, s, 0.0))
        return _

    lax.fori_loop(0, TP, project, 0)
    message(TAIL, kvx.at[pl.ds(GROUP, WINDOW)], kvx.at[pl.ds(0, WINDOW)], {"ep": lax.rem(me + 1, EP)})

    messages[STRIP_L].wait_recv()
    messages[STRIP_R].wait_recv()
    for number, k, part, to in (
        (STRIP_FL, 1, pl.ds(0, HALF), right), (STRIP_FR, 2, pl.ds(HALF, HALF), left),
    ):
        message(number, strips.at[k, strip, part], strips.at[3, strip, part], {"tp": to})

    messages[GATE_L].wait_recv()
    message(GATE_F, gate.at[1], gate.at[3], {"tp": right})
    messages[UP_R].wait_recv()
    message(UP_F, up.at[2], up.at[3], {"tp": left})

    messages[TAIL].wait_recv()

    band_lane = lax.broadcasted_iota(jnp.int32, (2 * WINDOW, 128), 1)
    band_key = band_lane < 64
    query_i = lax.broadcasted_iota(jnp.int32, (PAIRS * OWN, 2 * WINDOW), 0) & (WINDOW - 1)
    key_i = lax.broadcasted_iota(jnp.int32, (PAIRS * OWN, 2 * WINDOW), 1)
    distance = query_i + WINDOW - key_i
    in_window = (distance >= 0) & (distance < WINDOW)
    head_row = lax.broadcasted_iota(jnp.int32, (PAIRS * OWN, 1), 0)

    def sink(head):
        return sinks[0:1, head : head + 1]

    sink_of = [
        jnp.where(
            head_row < OWN, sink(odd), jnp.where(head_row < 2 * OWN, sink(2 + odd), sink(4 + odd))
        )
        for odd in (0, 1)
    ]

    def attend(n, _):
        band = kvx[pl.ds(pl.multiple_of(n * OWN, OWN), 2 * WINDOW), :].astype(f32)
        keys = jnp.where(band_key, band, 0.0)
        values = jnp.where(band_key, 0.0, band)
        key_sets = (keys.astype(bf16), pltpu.roll(keys, 64, 1).astype(bf16))
        value_sets = (pltpu.roll(values, 64, 1).astype(bf16), values.astype(bf16))
        allowed = in_window & (me * GROUP + n * OWN - WINDOW + key_i >= 0)
        q = qs[n]
        total = jnp.zeros((PAIRS * OWN, 128), f32)
        for odd in (0, 1):
            scores = lax.dot_general(
                q, key_sets[odd], (((1,), (1,)), ((), ())), preferred_element_type=f32
            ) * (1.0 / math.sqrt(HEAD_DIM))
            scores = jnp.where(allowed, scores, -jnp.inf)
            peak = jnp.maximum(jnp.max(scores, axis=-1, keepdims=True), sink_of[odd])
            e = jnp.exp(scores - peak)
            denominator = jnp.sum(e, axis=-1, keepdims=True) + jnp.exp(sink_of[odd] - peak)
            total = total + dot((e / denominator).astype(bf16), value_sets[odd])
        at = pl.ds(pl.multiple_of(n * OWN, OWN), OWN)
        for p in range(PAIRS):
            att[at, p * 128 : (p + 1) * 128] = total[p * OWN : (p + 1) * OWN].astype(bf16)
        return _

    lax.fori_loop(0, TP, attend, 0)

    loads["wo"].wait()

    def project_out(i, _):
        at = pl.ds(pl.multiple_of(i * OWN, OWN), OWN)
        for c in range(WIDTH // COLS):
            part = pl.ds(c * COLS, COLS)
            mix[at, part] = dot(att[at, :], wo_v[:, part]).astype(bf16)
        return _

    lax.fori_loop(0, TP, project_out, 0)

    all_blocks(out, arr, 0).wait_recv()

    def flatten(c, _):
        at = pl.ds(pl.multiple_of(c * COLS, COLS), COLS)
        rows[:, at] = arr[:, :, at].astype(f32).reshape(SLOTS, COLS).astype(bf16)
        return _

    lax.fori_loop(0, WIDTH // COLS, flatten, 0)

    def hidden(q):
        def body(i, _):
            at = pl.ds(pl.multiple_of(i * 256, 256), 256)
            g = dot(rows[at, :], gate[q])
            u = dot(rows[at, :], up[q])
            hid[at, q * PART : (q + 1) * PART] = (g / (1.0 + jnp.exp(-g)) * u).astype(bf16)
            return _

        lax.fori_loop(0, SLOTS // 256, body, 0)

    loads["gate"].wait()
    loads["up"].wait()
    hidden(0)
    messages[UP_L].wait_recv()
    hidden(1)
    messages[GATE_R].wait_recv()
    hidden(2)

    foreign = pl.ds(1, TP - 1)
    messages[STRIP_FL].wait_recv()
    messages[STRIP_FR].wait_recv()

    def spread(s, _):
        peer = me - place + lax.rem(place + s, ROW)
        pltpu.make_async_remote_copy(
            src_ref=strips.at[foreign, strip], dst_ref=strips.at[foreign, strip],
            send_sem=x_send.at[1 + CHUNKS], recv_sem=x_recv.at[1 + CHUNKS],
            device_id={"ep": peer}, device_id_type=MESH,
        ).start()
        return _

    lax.fori_loop(1, ROW, spread, 0)
    others = strips.at[foreign, pl.ds(0, SHARED - STRIP)]
    all_strips = pltpu.make_async_remote_copy(
        src_ref=others, dst_ref=others, send_sem=x_send.at[1 + CHUNKS], recv_sem=x_recv.at[1 + CHUNKS],
        device_id={"ep": lax.rem(me + 1, EP)}, device_id_type=MESH,
    )

    half = PART // 2

    def forward_down(c):
        messages[DOWN_L + c].wait_recv()
        message(
            DOWN_FL + c, down[c].at[pl.ds(PART, half)], down[c].at[pl.ds(3 * PART, half)], {"tp": right}
        )
        messages[DOWN_R + c].wait_recv()
        message(
            DOWN_FR + c, down[c].at[pl.ds(2 * PART + half, half)], down[c].at[pl.ds(3 * PART + half, half)],
            {"tp": left},
        )

    forward_down(0)
    send_down(1)
    send_down(2)
    messages[GATE_F].wait_recv()
    messages[UP_F].wait_recv()
    hidden(3)

    def finish(c):
        loads[f"down{c}"].wait()
        messages[DOWN_FL + c].wait_recv()
        messages[DOWN_FR + c].wait_recv()

        def body(i, _):
            at = pl.ds(pl.multiple_of(i * 256, 256), 256)
            got = dot(hid[at, :], down[c][...])
            blocks = pl.ds(i * (256 // CAP), 256 // CAP)
            res[c][blocks] = got.reshape(256 // CAP, CAP, CUTS[c]).astype(bf16)
            return _

        lax.fori_loop(0, SLOTS // 256, body, 0)
        exchange(lambda peer: res[c].at[peer], ret[c].at[me], 1 + c)
        ret[c][me] = res[c][me]

    def piece(ref, owner, columns):
        return ref.at[pl.ds(pl.multiple_of(owner * OWN, OWN), OWN), columns]

    low, high = pl.ds(0, HALF), pl.ds(HALF, HALF)

    finish(0)
    forward_down(1)
    send_down(3)
    for c in range(1, CHUNKS - 1):
        forward_down(c + 1)
        if c + 3 < CHUNKS:
            send_down(c + 3)
        if c + 1 == CHUNKS - 2:
            message(UNITS_L, piece(units, right, pl.ds(0, SHARED)), units_got.at[1], {"tp": right})
            message(UNITS_R, piece(units, left, pl.ds(0, SHARED)), units_got.at[2], {"tp": left})
            message(UNITS_F, piece(units, far, pl.ds(0, SHARED)), units_got.at[3], {"tp": far})
        if c + 1 < CHUNKS - 1:
            finish(c)

    message(MIX_FL, piece(mix, far, low), mix_far.at[0], {"tp": right})
    message(MIX_FR, piece(mix, far, high), mix_far.at[1], {"tp": left})
    message(MIX_L0, piece(mix, right, high), mix_got.at[0, :, high], {"tp": right})
    message(MIX_R0, piece(mix, left, low), mix_got.at[1, :, low], {"tp": left})
    finish(CHUNKS - 2)
    finish(CHUNKS - 1)

    def combine(c):
        all_blocks(res[c], ret[c], 1 + c).wait_recv()
        got = ret[c][...].astype(f32).reshape(SLOTS, CUTS[c]).astype(bf16)
        both = dot(weights[...], got)
        at = pl.ds(STARTS[c], CUTS[c])
        routed[:, at] = routed[:, at] + both[0:OWN] + both[OWN:]

    all_strips.wait_recv()
    for number in (UNITS_L, UNITS_R, UNITS_F):
        messages[number].wait_recv()
    for c in range(WIDTH // COLS):
        at = pl.ds(c * COLS, COLS)
        routed[:, at] = dot(units[own, :], strips[0, :, at]) + sum(
            dot(units_got[k], strips[k, :, at]) for k in range(1, TP)
        )

    def add_into(owner, columns, extra):
        at = pl.ds(pl.multiple_of(owner * OWN, OWN), OWN)
        mix[at, columns] = (mix[at, columns].astype(f32) + extra[...].astype(f32)).astype(bf16)

    combine(0)
    messages[MIX_FL].wait_recv()
    add_into(right, low, mix_far.at[0])
    message(MIX_L1, piece(mix, right, low), mix_got.at[0, :, low], {"tp": right})
    messages[MIX_FR].wait_recv()
    add_into(left, high, mix_far.at[1])
    message(MIX_R1, piece(mix, left, high), mix_got.at[1, :, high], {"tp": left})
    for c in range(1, CHUNKS):
        combine(c)
    expert_out[...] = routed[...].astype(bf16)

    for number in (MIX_L0, MIX_R0, MIX_L1, MIX_R1):
        messages[number].wait_recv()
    mixer_out[...] = (
        mix[own, :].astype(f32) + mix_got[0].astype(f32) + mix_got[1].astype(f32)
    ).astype(bf16)

    for copy in messages.values():
        copy.wait_send()
    all_blocks(out, arr, 0).wait_send()
    for c in range(CHUNKS):
        all_blocks(res[c], ret[c], 1 + c).wait_send()
    all_strips.wait_send()


def hand_on(mixer_in, expert_in, mixer_out, expert_out):
    mixer_out[...] = mixer_in[...]
    expert_out[...] = expert_in[...]


def local(
    mixer_input, expert_input, gain_mixer, gain_expert, query_weight, key_weight, value_weight,
    sink_logits, output_weight, expert_choice, route_weights, expert_gate, expert_up, expert_down,
    shared_gate, shared_up, shared_down,
):
    half_steps = (jnp.arange(128, dtype=jnp.int32) % (HEAD_DIM // 2)).astype(f32)
    steps = (rope_base ** (-(2.0 * half_steps) / HEAD_DIM))[None]
    hbm = pl.BlockSpec(memory_space=pltpu.HBM)
    vmem = pl.BlockSpec(memory_space=pltpu.VMEM)
    V = pltpu.VMEM
    scratch = [
        V((GROUP, WIDTH), bf16), V((GROUP, WIDTH), bf16), V((GROUP, WIDTH), bf16), V((GROUP, WIDTH), bf16),
        V((WIDTH, 384), bf16), V((128, WIDTH), bf16), V((384, WIDTH), bf16),
        V((WIDTH, SHARED), bf16), V((WIDTH, SHARED), bf16), V((TP, SHARED, WIDTH), bf16),
        V((TP, WIDTH, PART), bf16), V((TP, WIDTH, PART), bf16),
        V((EP, CAP, WIDTH), bf16), V((EP, CAP, WIDTH), bf16), V((SLOTS, WIDTH), bf16),
        V((SLOTS, TP * PART), bf16),
        V((1, WIDTH), f32), V((1, WIDTH), f32), V((1, 2 * PAIRS), f32), V((2, GROUP), jnp.int32), V((2, GROUP), f32),
        V((1, 128), f32), V((TP, PAIRS * OWN, 128), bf16), V((WINDOW + GROUP, 128), bf16), V((GROUP, 384), bf16),
        V((GROUP, WIDTH), bf16), V((2, OWN, HALF), bf16), V((2, OWN, WIDTH), bf16),
        V((GROUP, SHARED), bf16), V((TP, OWN, SHARED), bf16), V((OWN, WIDTH), f32),
        V((2 * OWN, SLOTS), bf16), V((SLOTS, OWN), bf16),
        *[V((TP * PART, cut), bf16) for cut in CUTS],
        *[V((EP, CAP, cut), bf16) for cut in CUTS],
        *[V((EP, CAP, cut), bf16) for cut in CUTS],
        pltpu.SemaphoreType.DMA((32,)), pltpu.SemaphoreType.DMA((MESSAGES,)),
        pltpu.SemaphoreType.DMA((MESSAGES,)), pltpu.SemaphoreType.DMA((2 + CHUNKS,)),
        pltpu.SemaphoreType.DMA((2 + CHUNKS,)),
    ]
    shape = jax.ShapeDtypeStruct((OWN, WIDTH), bf16)
    done = pl.pallas_call(
        kernel,
        out_shape=(shape, shape),
        in_specs=[hbm] * 18,
        out_specs=(vmem, vmem),
        scratch_shapes=scratch,
        compiler_params=pltpu.CompilerParams(
            collective_id=0, has_side_effects=True, vmem_limit_bytes=63 * 2**20
        ),
        name="everything",
    )(
        mixer_input, expert_input, query_weight, key_weight.T, value_weight.T, output_weight,
        shared_gate, shared_up, shared_down, expert_gate[0], expert_up[0], expert_down[0],
        gain_mixer[None], gain_expert[None], sink_logits[None], expert_choice.T, route_weights.T, steps,
    )
    return pl.pallas_call(
        hand_on, out_shape=(shape, shape), in_specs=[vmem] * 2, out_specs=(vmem, vmem), name="hand_on"
    )(*done)


def solution(mesh):
    placed = (
        P("ep", None),
        P("ep", None),
        P(),
        P(),
        P(None, "tp"),
        P(None, "tp"),
        P(None, "tp"),
        P("tp"),
        P("tp", None),
        P("ep", None),
        P("ep", None),
        P("ep", None, "tp"),
        P("ep", None, "tp"),
        P("ep", "tp", None),
        P(None, "tp"),
        P(None, "tp"),
        P("tp", None),
    )
    return jax.shard_map(
        local,
        mesh=mesh,
        in_specs=placed,
        out_specs=(P(("ep", "tp"), None), P(("ep", "tp"), None)),
        check_vma=False,
    )
```

```python
import functools
import math

import jax
import jax.numpy as jnp
from jax import lax
from jax.experimental import pallas as pl
from jax.experimental.pallas import tpu as pltpu
from jax.sharding import PartitionSpec as P

HEAD_DIM = 64
WINDOW = 128
MESH = pl.DeviceIdType.MESH

norm_eps = 1e-06
rope_base = 500000.0

GROUP = 512
OWN = 128
WIDTH = 2048
EP = 64
CAP = 8
SLOTS = EP * CAP
PART = 256
SHARED = 128
COLS = 512
CUTS = (128, 128, 128, 128) + (256,) * 6
CHUNKS = len(CUTS)
STARTS = tuple(sum(CUTS[:c]) for c in range(CHUNKS))
ROW = 8
STRIP = SHARED // ROW
HALF = WIDTH // 2
PAIRS = 3
TP = 4

GATE_L, UP_L, GATE_R, UP_R, TAIL = range(5)
GATE_F, UP_F = (20 + 4 * CHUNKS, 21 + 4 * CHUNKS), (22 + 4 * CHUNKS, 23 + 4 * CHUNKS)
STRIP_L, STRIP_R, STRIP_FL, STRIP_FR, UNITS_L, UNITS_R, UNITS_F = range(7, 14)
MIX_FL, MIX_FR, MIX_L0, MIX_L1, MIX_R0, MIX_R1 = range(14, 20)
DOWN_L, DOWN_R, DOWN_FL, DOWN_FR = (20 + CHUNKS * k for k in range(4))
MESSAGES = 24 + 4 * CHUNKS

f32, bf16 = jnp.float32, jnp.bfloat16


def dot(a, b):
    return jnp.dot(a, b, preferred_element_type=f32)


def kernel(
    xa, xb, wq, wk, wv, wo, sgate, sup, sdown, gate_in, up_in, down_in,
    gain_a_in, gain_b_in, sinks_in, choice_in, route_in, steps_in,
    mixer_out, expert_out,
    xa_v, xb_v, na, nb, wq_v, wkv_v, wo_v, sg_v, su_v, strips,
    gate, up, out, arr, rows, hid,
    gain_a, gain_b, sinks, choice_rows, route, steps,
    qs, kvx, att, mix, mix_far, mix_got, units, units_got, routed, weights, picks, mixer_v, expert_v,
    *rest,
):
    down, res, ret = (rest[k * CHUNKS : (k + 1) * CHUNKS] for k in range(3))
    load_sem, send_sem, recv_sem, x_send, x_recv, out_sem = rest[3 * CHUNKS :]
    me = lax.axis_index("ep")
    t = lax.axis_index("tp")
    right = lax.rem(t + 1, TP)
    left = lax.rem(t + TP - 1, TP)
    far = lax.rem(t + 2, TP)

    barrier = pltpu.get_barrier_semaphore()

    def greet(s, _):
        pl.semaphore_signal(barrier, inc=1, device_id={"ep": lax.rem(me + s, EP)}, device_id_type=MESH)
        return _

    for neighbour in (left, right, far):
        pl.semaphore_signal(barrier, inc=1, device_id={"tp": neighbour}, device_id_type=MESH)
    lax.fori_loop(1, EP, greet, 0)

    loads = {}

    def load(name, src, dst):
        copy = pltpu.make_async_copy(src, dst, load_sem.at[len(loads)])
        copy.start()
        loads[name] = copy

    load("choice", choice_in, choice_rows)
    load("route", route_in, route)
    load("gain_b", gain_b_in, gain_b)
    load("xb", xb, xb_v)
    load("gain_a", gain_a_in, gain_a)
    load("sinks", sinks_in, sinks)
    load("steps", steps_in, steps)
    load("sg", sgate, sg_v)
    load("su", sup, su_v)
    load("sd", sdown, strips.at[0])
    load("xa", xa, xa_v)
    load("wq", wq, wq_v)
    load("wk", wk, wkv_v.at[pl.ds(0, HEAD_DIM)])
    load("wv", wv, wkv_v.at[pl.ds(HEAD_DIM, HEAD_DIM)])
    load("wo", wo, wo_v)

    messages = {}

    def message(number, src, dst, to):
        copy = pltpu.make_async_remote_copy(
            src_ref=src, dst_ref=dst, send_sem=send_sem.at[number], recv_sem=recv_sem.at[number],
            device_id=to, device_id_type=MESH,
        )
        copy.start()
        messages[number] = copy

    pl.semaphore_wait(barrier, EP + 2)

    place = lax.rem(me, ROW)
    strip = pl.ds(pl.multiple_of(place * STRIP, STRIP), STRIP)
    message(STRIP_L, sdown.at[strip], strips.at[1, strip], {"tp": right})
    message(STRIP_R, sdown.at[strip], strips.at[2, strip], {"tp": left})
    message(GATE_L, gate_in, gate.at[1], {"tp": right})
    message(UP_R, up_in, up.at[2], {"tp": left})
    message(UP_L, up_in, up.at[1], {"tp": right})
    message(GATE_R, gate_in, gate.at[2], {"tp": left})

    def send_down(c):
        src = down_in.at[:, pl.ds(STARTS[c], CUTS[c])]
        message(DOWN_L + c, src, down[c].at[pl.ds(PART, PART)], {"tp": right})
        message(DOWN_R + c, src, down[c].at[pl.ds(2 * PART, PART)], {"tp": left})

    send_down(0)
    load("gate", gate_in, gate.at[0])
    load("up", up_in, up.at[0])
    for c in range(CHUNKS):
        load(f"down{c}", down_in.at[:, pl.ds(STARTS[c], CUTS[c])], down[c].at[pl.ds(0, PART)])

    own = pl.ds(pl.multiple_of(t * OWN, OWN), OWN)
    loads["choice"].wait()
    loads["route"].wait()
    row_a = choice_rows[0:1, own].astype(f32)
    row_b = choice_rows[1:2, own].astype(f32)
    down_i = lax.broadcasted_iota(jnp.int32, (OWN, OWN), 0)
    across_i = lax.broadcasted_iota(jnp.int32, (OWN, OWN), 1)

    def column(row):
        return jnp.sum(jnp.where(down_i == across_i, row, 0.0), axis=1, keepdims=True)

    col_a, col_b = column(row_a), column(row_b)

    def count(condition, axis):
        return jnp.sum(jnp.where(condition, 1.0, 0.0).astype(f32), axis=axis, keepdims=True)

    before = down_i < across_i
    after = down_i > across_i
    slot_row_a = row_a * CAP + count((col_a == row_a) & before, 0)
    slot_row_b = row_b * CAP + count(col_a == row_b, 0) + count((col_b == row_b) & before, 0)
    slot_col_a = col_a * CAP + count((col_a == row_a) & after, 1)
    slot_col_b = col_b * CAP + count(col_b == row_a, 1) + count((col_b == row_b) & after, 1)
    slot_i = lax.broadcasted_iota(jnp.int32, (SLOTS, OWN), 0).astype(f32)
    picks[...] = jnp.where((slot_i == slot_row_a) | (slot_i == slot_row_b), 1.0, 0.0).astype(bf16)
    slot_j = lax.broadcasted_iota(jnp.int32, (OWN, SLOTS), 1).astype(f32)
    share = jnp.where(slot_j == slot_col_a, column(route[0:1, own]), 0.0) + jnp.where(
        slot_j == slot_col_b, column(route[1:2, own]), 0.0
    )
    coarse = share.astype(bf16)
    weights[0:OWN, :] = coarse
    weights[OWN:, :] = (share - coarse.astype(f32)).astype(bf16)

    def normalise(src, dst, gain, start, count_of):
        step = 32

        def body(i, _):
            at = pl.ds(pl.multiple_of(start + i * step, step), step)
            wide = src[at, :].astype(f32)
            scale = lax.rsqrt(jnp.mean(wide * wide, axis=-1, keepdims=True) + norm_eps)
            dst[at, :] = (wide * scale * gain[...]).astype(bf16)
            return _

        lax.fori_loop(0, count_of // step, body, 0)

    loads["gain_b"].wait()
    loads["xb"].wait()
    normalise(xb_v, nb, gain_b, t * OWN, OWN)

    def gather(c, _):
        at = pl.ds(pl.multiple_of(c * COLS, COLS), COLS)
        got = dot(picks[...], nb[own, at])
        out[:, :, at] = got.reshape(EP, CAP, COLS).astype(bf16)
        return _

    lax.fori_loop(0, WIDTH // COLS, gather, 0)

    def exchange(src_of, dst, number):
        def body(s, _):
            peer = lax.rem(me + s, EP)
            pltpu.make_async_remote_copy(
                src_ref=src_of(peer), dst_ref=dst, send_sem=x_send.at[number], recv_sem=x_recv.at[number],
                device_id={"ep": peer}, device_id_type=MESH,
            ).start()
            return _

        lax.fori_loop(1, EP, body, 0)

    def all_blocks(src, dst, number):
        most = pl.ds(0, EP - 1)
        return pltpu.make_async_remote_copy(
            src_ref=src.at[most], dst_ref=dst.at[most], send_sem=x_send.at[number], recv_sem=x_recv.at[number],
            device_id={"ep": lax.rem(me + 1, EP)}, device_id_type=MESH,
        )

    exchange(lambda peer: out.at[peer], arr.at[me], 0)
    arr[me] = out[me]

    normalise(xb_v, nb, gain_b, 0, GROUP)
    for name in ("sg", "su", "sd"):
        loads[name].wait()

    def shared(i, _):
        at = pl.ds(pl.multiple_of(i * OWN, OWN), OWN)
        g = dot(nb[at, :], sg_v[...])
        u = dot(nb[at, :], su_v[...])
        units[at, :] = (g / (1.0 + jnp.exp(-g)) * u).astype(bf16)
        return _

    lax.fori_loop(0, TP, shared, 0)

    for name in ("xa", "wq", "wk", "wv", "gain_a", "sinks", "steps"):
        loads[name].wait()
    normalise(xa_v, na, gain_a, 0, GROUP)
    lane = lax.broadcasted_iota(jnp.int32, (OWN, 128), 1)
    first_half = (lane & 63) < 32
    is_key = lane < 64

    def turn(value, c, s):
        value = value.astype(bf16).astype(f32)
        partner = jnp.where(first_half, pltpu.roll(value, 96, 1), pltpu.roll(value, 32, 1))
        return (value * c + partner * s).astype(bf16)

    def project(i, _):
        at = pl.ds(pl.multiple_of(i * OWN, OWN), OWN)
        position = me * GROUP + i * OWN + down_i
        angles = position.astype(f32) * steps[...]
        c, s = jnp.cos(angles), jnp.sin(angles)
        s = jnp.where(first_half, -s, s)
        q = dot(na[at, :], wq_v[...])
        for p in range(PAIRS):
            qs[i, p * OWN : (p + 1) * OWN, :] = turn(q[:, p * 128 : (p + 1) * 128], c, s)
        kv = lax.dot_general(na[at, :], wkv_v[...], (((1,), (1,)), ((), ())), preferred_element_type=f32)
        after_tail = pl.ds(pl.multiple_of(WINDOW + i * OWN, OWN), OWN)
        kvx[after_tail, :] = turn(kv, jnp.where(is_key, c, 1.0), jnp.where(is_key, s, 0.0))
        return _

    lax.fori_loop(0, TP, project, 0)
    message(TAIL, kvx.at[pl.ds(GROUP, WINDOW)], kvx.at[pl.ds(0, WINDOW)], {"ep": lax.rem(me + 1, EP)})

    messages[STRIP_L].wait_recv()
    messages[STRIP_R].wait_recv()
    for number, k, part, to in (
        (STRIP_FL, 1, pl.ds(0, HALF), right), (STRIP_FR, 2, pl.ds(HALF, HALF), left),
    ):
        message(number, strips.at[k, strip, part], strips.at[3, strip, part], {"tp": to})

    messages[GATE_L].wait_recv()
    halves = [pl.ds(0, PART // 2), pl.ds(PART // 2, PART // 2)]
    for number, units_at in zip(GATE_F, halves):
        message(number, gate.at[1, :, units_at], gate.at[3, :, units_at], {"tp": right})
    messages[UP_R].wait_recv()
    for number, units_at in zip(UP_F, halves):
        message(number, up.at[2, :, units_at], up.at[3, :, units_at], {"tp": left})

    messages[TAIL].wait_recv()

    band_lane = lax.broadcasted_iota(jnp.int32, (2 * WINDOW, 128), 1)
    band_key = band_lane < 64
    query_i = lax.broadcasted_iota(jnp.int32, (PAIRS * OWN, 2 * WINDOW), 0) & (WINDOW - 1)
    key_i = lax.broadcasted_iota(jnp.int32, (PAIRS * OWN, 2 * WINDOW), 1)
    distance = query_i + WINDOW - key_i
    in_window = (distance >= 0) & (distance < WINDOW)
    head_row = lax.broadcasted_iota(jnp.int32, (PAIRS * OWN, 1), 0)

    def sink(head):
        return sinks[0:1, head : head + 1]

    sink_of = [
        jnp.where(
            head_row < OWN, sink(odd), jnp.where(head_row < 2 * OWN, sink(2 + odd), sink(4 + odd))
        )
        for odd in (0, 1)
    ]

    def attend(n, _):
        band = kvx[pl.ds(pl.multiple_of(n * OWN, OWN), 2 * WINDOW), :].astype(f32)
        keys = jnp.where(band_key, band, 0.0)
        values = jnp.where(band_key, 0.0, band)
        key_sets = (keys.astype(bf16), pltpu.roll(keys, 64, 1).astype(bf16))
        value_sets = (pltpu.roll(values, 64, 1).astype(bf16), values.astype(bf16))
        allowed = in_window & (me * GROUP + n * OWN - WINDOW + key_i >= 0)
        q = qs[n]
        total = jnp.zeros((PAIRS * OWN, 128), f32)
        for odd in (0, 1):
            scores = lax.dot_general(
                q, key_sets[odd], (((1,), (1,)), ((), ())), preferred_element_type=f32
            ) * (1.0 / math.sqrt(HEAD_DIM))
            scores = jnp.where(allowed, scores, -jnp.inf)
            peak = jnp.maximum(jnp.max(scores, axis=-1, keepdims=True), sink_of[odd])
            e = jnp.exp(scores - peak)
            denominator = jnp.sum(e, axis=-1, keepdims=True) + jnp.exp(sink_of[odd] - peak)
            total = total + dot((e / denominator).astype(bf16), value_sets[odd])
        at = pl.ds(pl.multiple_of(n * OWN, OWN), OWN)
        for p in range(PAIRS):
            att[at, p * 128 : (p + 1) * 128] = total[p * OWN : (p + 1) * OWN].astype(bf16)
        return _

    lax.fori_loop(0, TP, attend, 0)

    loads["wo"].wait()

    def project_out(i, _):
        at = pl.ds(pl.multiple_of(i * OWN, OWN), OWN)
        for c in range(WIDTH // COLS):
            part = pl.ds(c * COLS, COLS)
            mix[at, part] = dot(att[at, :], wo_v[:, part]).astype(bf16)
        return _

    lax.fori_loop(0, TP, project_out, 0)

    all_blocks(out, arr, 0).wait_recv()

    def flatten(c, _):
        at = pl.ds(pl.multiple_of(c * COLS, COLS), COLS)
        rows[:, at] = arr[:, :, at].astype(f32).reshape(SLOTS, COLS).astype(bf16)
        return _

    lax.fori_loop(0, WIDTH // COLS, flatten, 0)

    def hidden(q, low_unit=0, high_unit=PART):
        def body(i, _):
            at = pl.ds(pl.multiple_of(i * 256, 256), 256)
            g = dot(rows[at, :], gate[q, :, low_unit:high_unit])
            u = dot(rows[at, :], up[q, :, low_unit:high_unit])
            hid[at, q * PART + low_unit : q * PART + high_unit] = (g / (1.0 + jnp.exp(-g)) * u).astype(bf16)
            return _

        lax.fori_loop(0, SLOTS // 256, body, 0)

    loads["gate"].wait()
    loads["up"].wait()
    hidden(0)
    messages[UP_L].wait_recv()
    hidden(1)
    messages[GATE_R].wait_recv()
    hidden(2)

    foreign = pl.ds(1, TP - 1)
    messages[STRIP_FL].wait_recv()
    messages[STRIP_FR].wait_recv()

    def spread(s, _):
        peer = me - place + lax.rem(place + s, ROW)
        pltpu.make_async_remote_copy(
            src_ref=strips.at[foreign, strip], dst_ref=strips.at[foreign, strip],
            send_sem=x_send.at[1 + CHUNKS], recv_sem=x_recv.at[1 + CHUNKS],
            device_id={"ep": peer}, device_id_type=MESH,
        ).start()
        return _

    lax.fori_loop(1, ROW, spread, 0)
    others = strips.at[foreign, pl.ds(0, SHARED - STRIP)]
    all_strips = pltpu.make_async_remote_copy(
        src_ref=others, dst_ref=others, send_sem=x_send.at[1 + CHUNKS], recv_sem=x_recv.at[1 + CHUNKS],
        device_id={"ep": lax.rem(me + 1, EP)}, device_id_type=MESH,
    )

    half = PART // 2

    def forward_down(c):
        messages[DOWN_L + c].wait_recv()
        message(
            DOWN_FL + c, down[c].at[pl.ds(PART, half)], down[c].at[pl.ds(3 * PART, half)], {"tp": right}
        )
        messages[DOWN_R + c].wait_recv()
        message(
            DOWN_FR + c, down[c].at[pl.ds(2 * PART + half, half)], down[c].at[pl.ds(3 * PART + half, half)],
            {"tp": left},
        )

    forward_down(0)
    send_down(1)
    send_down(2)
    for k in (0, 1):
        messages[GATE_F[k]].wait_recv()
        messages[UP_F[k]].wait_recv()
        hidden(3, k * (PART // 2), (k + 1) * (PART // 2))

    def finish(c):
        loads[f"down{c}"].wait()
        messages[DOWN_FL + c].wait_recv()
        messages[DOWN_FR + c].wait_recv()

        def body(i, _):
            at = pl.ds(pl.multiple_of(i * 256, 256), 256)
            got = dot(hid[at, :], down[c][...])
            blocks = pl.ds(i * (256 // CAP), 256 // CAP)
            res[c][blocks] = got.reshape(256 // CAP, CAP, CUTS[c]).astype(bf16)
            return _

        lax.fori_loop(0, SLOTS // 256, body, 0)
        exchange(lambda peer: res[c].at[peer], ret[c].at[me], 1 + c)
        ret[c][me] = res[c][me]

    def piece(ref, owner, columns):
        return ref.at[pl.ds(pl.multiple_of(owner * OWN, OWN), OWN), columns]

    low, high = pl.ds(0, HALF), pl.ds(HALF, HALF)

    finish(0)
    forward_down(1)
    send_down(3)
    for c in range(1, CHUNKS - 1):
        forward_down(c + 1)
        if c + 3 < CHUNKS:
            send_down(c + 3)
        if c + 1 == CHUNKS - 2:
            message(UNITS_L, piece(units, right, pl.ds(0, SHARED)), units_got.at[1], {"tp": right})
            message(UNITS_R, piece(units, left, pl.ds(0, SHARED)), units_got.at[2], {"tp": left})
            message(UNITS_F, piece(units, far, pl.ds(0, SHARED)), units_got.at[3], {"tp": far})
        if c + 1 < CHUNKS - 1:
            finish(c)

    message(MIX_FL, piece(mix, far, low), mix_far.at[0], {"tp": right})
    message(MIX_FR, piece(mix, far, high), mix_far.at[1], {"tp": left})
    message(MIX_L0, piece(mix, right, high), mix_got.at[0, :, high], {"tp": right})
    message(MIX_R0, piece(mix, left, low), mix_got.at[1, :, low], {"tp": left})
    finish(CHUNKS - 2)
    finish(CHUNKS - 1)

    leaving = []

    def leave(src, dst):
        copy = pltpu.make_async_copy(src, dst, out_sem.at[len(leaving)])
        copy.start()
        leaving.append(copy)

    def combine(c):
        all_blocks(res[c], ret[c], 1 + c).wait_recv()
        got = ret[c][...].astype(f32).reshape(SLOTS, CUTS[c]).astype(bf16)
        both = dot(weights[...], got)
        at = pl.ds(STARTS[c], CUTS[c])
        expert_v[:, at] = (routed[:, at] + both[0:OWN] + both[OWN:]).astype(bf16)
        leave(expert_v.at[:, at], expert_out.at[:, at])

    all_strips.wait_recv()
    for number in (UNITS_L, UNITS_R, UNITS_F):
        messages[number].wait_recv()
    for c in range(WIDTH // COLS):
        at = pl.ds(c * COLS, COLS)
        routed[:, at] = dot(units[own, :], strips[0, :, at]) + sum(
            dot(units_got[k], strips[k, :, at]) for k in range(1, TP)
        )

    def add_into(owner, columns, extra):
        at = pl.ds(pl.multiple_of(owner * OWN, OWN), OWN)
        mix[at, columns] = (mix[at, columns].astype(f32) + extra[...].astype(f32)).astype(bf16)

    combine(0)
    messages[MIX_FL].wait_recv()
    add_into(right, low, mix_far.at[0])
    message(MIX_L1, piece(mix, right, low), mix_got.at[0, :, low], {"tp": right})
    messages[MIX_FR].wait_recv()
    add_into(left, high, mix_far.at[1])
    message(MIX_R1, piece(mix, left, high), mix_got.at[1, :, high], {"tp": left})
    for c in range(1, CHUNKS - 1):
        combine(c)

    for number in (MIX_L0, MIX_R0, MIX_L1, MIX_R1):
        messages[number].wait_recv()
    mixer_v[...] = (
        mix[own, :].astype(f32) + mix_got[0].astype(f32) + mix_got[1].astype(f32)
    ).astype(bf16)
    leave(mixer_v, mixer_out)
    combine(CHUNKS - 1)

    for copy in leaving:
        copy.wait()
    for copy in messages.values():
        copy.wait_send()
    all_blocks(out, arr, 0).wait_send()
    for c in range(CHUNKS):
        all_blocks(res[c], ret[c], 1 + c).wait_send()
    all_strips.wait_send()


def hand_on(mixer_in, expert_in, mixer_out, expert_out, held, in_sem, out_sem):
    pieces = [(mixer_in, mixer_out, 0), (expert_in, expert_out, 0), (mixer_in, mixer_out, 1), (expert_in, expert_out, 1)]
    arriving, leaving = [], []
    for k, (src, _, half) in enumerate(pieces):
        copy = pltpu.make_async_copy(src.at[pl.ds(half * 64, 64)], held.at[k], in_sem.at[k])
        copy.start()
        arriving.append(copy)
    for k, (_, dst, half) in enumerate(pieces):
        arriving[k].wait()
        copy = pltpu.make_async_copy(held.at[k], dst.at[pl.ds(half * 64, 64)], out_sem.at[k])
        copy.start()
        leaving.append(copy)
    for copy in leaving:
        copy.wait()


def local(
    mixer_input, expert_input, gain_mixer, gain_expert, query_weight, key_weight, value_weight,
    sink_logits, output_weight, expert_choice, route_weights, expert_gate, expert_up, expert_down,
    shared_gate, shared_up, shared_down,
):
    half_steps = (jnp.arange(128, dtype=jnp.int32) % (HEAD_DIM // 2)).astype(f32)
    steps = (rope_base ** (-(2.0 * half_steps) / HEAD_DIM))[None]
    hbm = pl.BlockSpec(memory_space=pltpu.HBM)
    V = pltpu.VMEM
    scratch = [
        V((GROUP, WIDTH), bf16), V((GROUP, WIDTH), bf16), V((GROUP, WIDTH), bf16), V((GROUP, WIDTH), bf16),
        V((WIDTH, 384), bf16), V((128, WIDTH), bf16), V((384, WIDTH), bf16),
        V((WIDTH, SHARED), bf16), V((WIDTH, SHARED), bf16), V((TP, SHARED, WIDTH), bf16),
        V((TP, WIDTH, PART), bf16), V((TP, WIDTH, PART), bf16),
        V((EP, CAP, WIDTH), bf16), V((EP, CAP, WIDTH), bf16), V((SLOTS, WIDTH), bf16),
        V((SLOTS, TP * PART), bf16),
        V((1, WIDTH), f32), V((1, WIDTH), f32), V((1, 2 * PAIRS), f32), V((2, GROUP), jnp.int32), V((2, GROUP), f32),
        V((1, 128), f32), V((TP, PAIRS * OWN, 128), bf16), V((WINDOW + GROUP, 128), bf16), V((GROUP, 384), bf16),
        V((GROUP, WIDTH), bf16), V((2, OWN, HALF), bf16), V((2, OWN, WIDTH), bf16),
        V((GROUP, SHARED), bf16), V((TP, OWN, SHARED), bf16), V((OWN, WIDTH), f32),
        V((2 * OWN, SLOTS), bf16), V((SLOTS, OWN), bf16),
        V((OWN, WIDTH), bf16), V((OWN, WIDTH), bf16),
        *[V((TP * PART, cut), bf16) for cut in CUTS],
        *[V((EP, CAP, cut), bf16) for cut in CUTS],
        *[V((EP, CAP, cut), bf16) for cut in CUTS],
        pltpu.SemaphoreType.DMA((32,)), pltpu.SemaphoreType.DMA((MESSAGES,)),
        pltpu.SemaphoreType.DMA((MESSAGES,)), pltpu.SemaphoreType.DMA((2 + CHUNKS,)),
        pltpu.SemaphoreType.DMA((2 + CHUNKS,)), pltpu.SemaphoreType.DMA((1 + CHUNKS,)),
    ]
    shape = jax.ShapeDtypeStruct((OWN, WIDTH), bf16)
    done = pl.pallas_call(
        kernel,
        out_shape=(shape, shape),
        in_specs=[hbm] * 18,
        out_specs=(hbm, hbm),
        scratch_shapes=scratch,
        compiler_params=pltpu.CompilerParams(
            collective_id=0, has_side_effects=True, vmem_limit_bytes=63 * 2**20
        ),
        name="everything",
    )(
        mixer_input, expert_input, query_weight, key_weight.T, value_weight.T, output_weight,
        shared_gate, shared_up, shared_down, expert_gate[0], expert_up[0], expert_down[0],
        gain_mixer[None], gain_expert[None], sink_logits[None], expert_choice.T, route_weights.T, steps,
    )
    return pl.pallas_call(
        hand_on, out_shape=(shape, shape), in_specs=[hbm] * 2, out_specs=(hbm, hbm), name="hand_on",
        scratch_shapes=[V((4, OWN // 2, WIDTH), bf16), pltpu.SemaphoreType.DMA((4,)), pltpu.SemaphoreType.DMA((4,))],
    )(*done)


def solution(mesh):
    placed = (
        P("ep", None),
        P("ep", None),
        P(),
        P(),
        P(None, "tp"),
        P(None, "tp"),
        P(None, "tp"),
        P("tp"),
        P("tp", None),
        P("ep", None),
        P("ep", None),
        P("ep", None, "tp"),
        P("ep", None, "tp"),
        P("ep", "tp", None),
        P(None, "tp"),
        P(None, "tp"),
        P("tp", None),
    )
    return jax.shard_map(
        local,
        mesh=mesh,
        in_specs=placed,
        out_specs=(P(("ep", "tp"), None), P(("ep", "tp"), None)),
        check_vma=False,
    )
```

```python
import functools
import math

import jax
import jax.numpy as jnp
from jax import lax
from jax.experimental import pallas as pl
from jax.experimental.pallas import tpu as pltpu
from jax.sharding import PartitionSpec as P

HEAD_DIM = 64
WINDOW = 128
MESH = pl.DeviceIdType.MESH

norm_eps = 1e-06
rope_base = 500000.0

GROUP = 512
OWN = 128
WIDTH = 2048
EP = 64
CAP = 8
SLOTS = EP * CAP
PART = 256
SHARED = 128
COLS = 512
CUTS = (128, 128, 128, 128) + (256,) * 6
CHUNKS = len(CUTS)
STARTS = tuple(sum(CUTS[:c]) for c in range(CHUNKS))
ROW = 8
STRIP = SHARED // ROW
HALF = WIDTH // 2
DEPTHS = ((0, 1536), (1536, WIDTH))
PAIRS = 3
TP = 4

GATE_L, UP_L, GATE_R, UP_R, TAIL = range(5)
GATE_F, UP_F = (20 + 4 * CHUNKS, 21 + 4 * CHUNKS), (22 + 4 * CHUNKS, 23 + 4 * CHUNKS)
STRIP_L, STRIP_R, STRIP_FL, STRIP_FR, UNITS_L, UNITS_R, UNITS_F = range(7, 14)
MIX_FL, MIX_FR, MIX_L0, MIX_L1, MIX_R0, MIX_R1 = range(14, 20)
DOWN_L, DOWN_R, DOWN_FL, DOWN_FR = (20 + CHUNKS * k for k in range(4))
MESSAGES = 24 + 4 * CHUNKS

f32, bf16 = jnp.float32, jnp.bfloat16


def dot(a, b):
    return jnp.dot(a, b, preferred_element_type=f32)


def kernel(
    xa, xb, wq, wk, wv, wo, sgate, sup, sdown, gate_in, up_in, down_in,
    gain_a_in, gain_b_in, sinks_in, choice_in, route_in, steps_in,
    mixer_out, expert_out,
    xa_v, xb_v, na, nb, wq_v, wkv_v, wo_v, sg_v, su_v, strips,
    gate, up, out, arr, rows, hid,
    gain_a, gain_b, sinks, choice_rows, route, steps,
    qs, kvx, att, mix, mix_far, mix_got, units, units_got, routed, weights, picks, mixer_v, expert_v, gate_sum, up_sum, first_sum,
    *rest,
):
    down, res, ret = (rest[k * CHUNKS : (k + 1) * CHUNKS] for k in range(3))
    load_sem, send_sem, recv_sem, x_send, x_recv, out_sem = rest[3 * CHUNKS :]
    me = lax.axis_index("ep")
    t = lax.axis_index("tp")
    right = lax.rem(t + 1, TP)
    left = lax.rem(t + TP - 1, TP)
    far = lax.rem(t + 2, TP)

    barrier = pltpu.get_barrier_semaphore()

    def greet(s, _):
        pl.semaphore_signal(barrier, inc=1, device_id={"ep": lax.rem(me + s, EP)}, device_id_type=MESH)
        return _

    for neighbour in (left, right, far):
        pl.semaphore_signal(barrier, inc=1, device_id={"tp": neighbour}, device_id_type=MESH)
    lax.fori_loop(1, EP, greet, 0)

    loads = {}

    def load(name, src, dst):
        copy = pltpu.make_async_copy(src, dst, load_sem.at[len(loads)])
        copy.start()
        loads[name] = copy

    load("choice", choice_in, choice_rows)
    load("route", route_in, route)
    load("gain_b", gain_b_in, gain_b)
    load("xb", xb, xb_v)
    load("gain_a", gain_a_in, gain_a)
    load("sinks", sinks_in, sinks)
    load("steps", steps_in, steps)
    load("sg", sgate, sg_v)
    load("su", sup, su_v)
    load("sd", sdown, strips.at[0])
    load("xa", xa, xa_v)
    load("wq", wq, wq_v)
    load("wk", wk, wkv_v.at[pl.ds(0, HEAD_DIM)])
    load("wv", wv, wkv_v.at[pl.ds(HEAD_DIM, HEAD_DIM)])
    load("wo", wo, wo_v)

    messages = {}

    def message(number, src, dst, to):
        copy = pltpu.make_async_remote_copy(
            src_ref=src, dst_ref=dst, send_sem=send_sem.at[number], recv_sem=recv_sem.at[number],
            device_id=to, device_id_type=MESH,
        )
        copy.start()
        messages[number] = copy

    pl.semaphore_wait(barrier, EP + 2)

    place = lax.rem(me, ROW)
    strip = pl.ds(pl.multiple_of(place * STRIP, STRIP), STRIP)
    message(STRIP_L, sdown.at[strip], strips.at[1, strip], {"tp": right})
    message(STRIP_R, sdown.at[strip], strips.at[2, strip], {"tp": left})
    message(GATE_L, gate_in, gate.at[1], {"tp": right})
    message(UP_R, up_in, up.at[2], {"tp": left})
    message(UP_L, up_in, up.at[1], {"tp": right})
    message(GATE_R, gate_in, gate.at[2], {"tp": left})

    def send_down(c):
        src = down_in.at[:, pl.ds(STARTS[c], CUTS[c])]
        message(DOWN_L + c, src, down[c].at[pl.ds(PART, PART)], {"tp": right})
        message(DOWN_R + c, src, down[c].at[pl.ds(2 * PART, PART)], {"tp": left})

    send_down(0)
    load("gate", gate_in, gate.at[0])
    load("up", up_in, up.at[0])
    for c in range(CHUNKS):
        load(f"down{c}", down_in.at[:, pl.ds(STARTS[c], CUTS[c])], down[c].at[pl.ds(0, PART)])

    own = pl.ds(pl.multiple_of(t * OWN, OWN), OWN)
    loads["choice"].wait()
    loads["route"].wait()
    row_a = choice_rows[0:1, own].astype(f32)
    row_b = choice_rows[1:2, own].astype(f32)
    down_i = lax.broadcasted_iota(jnp.int32, (OWN, OWN), 0)
    across_i = lax.broadcasted_iota(jnp.int32, (OWN, OWN), 1)

    def column(row):
        return jnp.sum(jnp.where(down_i == across_i, row, 0.0), axis=1, keepdims=True)

    col_a, col_b = column(row_a), column(row_b)

    def count(condition, axis):
        return jnp.sum(jnp.where(condition, 1.0, 0.0).astype(f32), axis=axis, keepdims=True)

    before = down_i < across_i
    after = down_i > across_i
    slot_row_a = row_a * CAP + count((col_a == row_a) & before, 0)
    slot_row_b = row_b * CAP + count(col_a == row_b, 0) + count((col_b == row_b) & before, 0)
    slot_col_a = col_a * CAP + count((col_a == row_a) & after, 1)
    slot_col_b = col_b * CAP + count(col_b == row_a, 1) + count((col_b == row_b) & after, 1)
    slot_i = lax.broadcasted_iota(jnp.int32, (SLOTS, OWN), 0).astype(f32)
    picks[...] = jnp.where((slot_i == slot_row_a) | (slot_i == slot_row_b), 1.0, 0.0).astype(bf16)
    slot_j = lax.broadcasted_iota(jnp.int32, (OWN, SLOTS), 1).astype(f32)
    share = jnp.where(slot_j == slot_col_a, column(route[0:1, own]), 0.0) + jnp.where(
        slot_j == slot_col_b, column(route[1:2, own]), 0.0
    )
    coarse = share.astype(bf16)
    weights[0:OWN, :] = coarse
    weights[OWN:, :] = (share - coarse.astype(f32)).astype(bf16)

    def normalise(src, dst, gain, start, count_of):
        step = 32

        def body(i, _):
            at = pl.ds(pl.multiple_of(start + i * step, step), step)
            wide = src[at, :].astype(f32)
            scale = lax.rsqrt(jnp.mean(wide * wide, axis=-1, keepdims=True) + norm_eps)
            dst[at, :] = (wide * scale * gain[...]).astype(bf16)
            return _

        lax.fori_loop(0, count_of // step, body, 0)

    loads["gain_b"].wait()
    loads["xb"].wait()
    normalise(xb_v, nb, gain_b, t * OWN, OWN)

    def gather(c, _):
        at = pl.ds(pl.multiple_of(c * COLS, COLS), COLS)
        got = dot(picks[...], nb[own, at])
        out[:, :, at] = got.reshape(EP, CAP, COLS).astype(bf16)
        return _

    lax.fori_loop(0, WIDTH // COLS, gather, 0)

    def exchange(src_of, dst, number):
        def body(s, _):
            peer = lax.rem(me + s, EP)
            pltpu.make_async_remote_copy(
                src_ref=src_of(peer), dst_ref=dst, send_sem=x_send.at[number], recv_sem=x_recv.at[number],
                device_id={"ep": peer}, device_id_type=MESH,
            ).start()
            return _

        lax.fori_loop(1, EP, body, 0)

    def all_blocks(src, dst, number):
        most = pl.ds(0, EP - 1)
        return pltpu.make_async_remote_copy(
            src_ref=src.at[most], dst_ref=dst.at[most], send_sem=x_send.at[number], recv_sem=x_recv.at[number],
            device_id={"ep": lax.rem(me + 1, EP)}, device_id_type=MESH,
        )

    exchange(lambda peer: out.at[peer], arr.at[me], 0)
    arr[me] = out[me]

    normalise(xb_v, nb, gain_b, 0, GROUP)
    for name in ("sg", "su", "sd"):
        loads[name].wait()

    def shared(i, _):
        at = pl.ds(pl.multiple_of(i * OWN, OWN), OWN)
        g = dot(nb[at, :], sg_v[...])
        u = dot(nb[at, :], su_v[...])
        units[at, :] = (g / (1.0 + jnp.exp(-g)) * u).astype(bf16)
        return _

    lax.fori_loop(0, TP, shared, 0)

    for name in ("xa", "wq", "wk", "wv", "gain_a", "sinks", "steps"):
        loads[name].wait()
    normalise(xa_v, na, gain_a, 0, GROUP)
    lane = lax.broadcasted_iota(jnp.int32, (OWN, 128), 1)
    first_half = (lane & 63) < 32
    is_key = lane < 64

    def turn(value, c, s):
        value = value.astype(bf16).astype(f32)
        partner = jnp.where(first_half, pltpu.roll(value, 96, 1), pltpu.roll(value, 32, 1))
        return (value * c + partner * s).astype(bf16)

    def project(i, _):
        at = pl.ds(pl.multiple_of(i * OWN, OWN), OWN)
        position = me * GROUP + i * OWN + down_i
        angles = position.astype(f32) * steps[...]
        c, s = jnp.cos(angles), jnp.sin(angles)
        s = jnp.where(first_half, -s, s)
        q = dot(na[at, :], wq_v[...])
        for p in range(PAIRS):
            qs[i, p * OWN : (p + 1) * OWN, :] = turn(q[:, p * 128 : (p + 1) * 128], c, s)
        kv = lax.dot_general(na[at, :], wkv_v[...], (((1,), (1,)), ((), ())), preferred_element_type=f32)
        after_tail = pl.ds(pl.multiple_of(WINDOW + i * OWN, OWN), OWN)
        kvx[after_tail, :] = turn(kv, jnp.where(is_key, c, 1.0), jnp.where(is_key, s, 0.0))
        return _

    lax.fori_loop(0, TP, project, 0)
    message(TAIL, kvx.at[pl.ds(GROUP, WINDOW)], kvx.at[pl.ds(0, WINDOW)], {"ep": lax.rem(me + 1, EP)})

    messages[STRIP_L].wait_recv()
    messages[STRIP_R].wait_recv()
    for number, k, part, to in (
        (STRIP_FL, 1, pl.ds(0, HALF), right), (STRIP_FR, 2, pl.ds(HALF, HALF), left),
    ):
        message(number, strips.at[k, strip, part], strips.at[3, strip, part], {"tp": to})

    messages[GATE_L].wait_recv()
    for number, (top, bottom) in zip(GATE_F, DEPTHS):
        depth = pl.ds(top, bottom - top)
        message(number, gate.at[1, depth], gate.at[3, depth], {"tp": right})
    messages[UP_R].wait_recv()
    for number, (top, bottom) in zip(UP_F, DEPTHS):
        depth = pl.ds(top, bottom - top)
        message(number, up.at[2, depth], up.at[3, depth], {"tp": left})

    messages[TAIL].wait_recv()

    band_lane = lax.broadcasted_iota(jnp.int32, (2 * WINDOW, 128), 1)
    band_key = band_lane < 64
    query_i = lax.broadcasted_iota(jnp.int32, (PAIRS * OWN, 2 * WINDOW), 0) & (WINDOW - 1)
    key_i = lax.broadcasted_iota(jnp.int32, (PAIRS * OWN, 2 * WINDOW), 1)
    distance = query_i + WINDOW - key_i
    in_window = (distance >= 0) & (distance < WINDOW)
    head_row = lax.broadcasted_iota(jnp.int32, (PAIRS * OWN, 1), 0)

    def sink(head):
        return sinks[0:1, head : head + 1]

    sink_of = [
        jnp.where(
            head_row < OWN, sink(odd), jnp.where(head_row < 2 * OWN, sink(2 + odd), sink(4 + odd))
        )
        for odd in (0, 1)
    ]

    def attend(n, _):
        band = kvx[pl.ds(pl.multiple_of(n * OWN, OWN), 2 * WINDOW), :].astype(f32)
        keys = jnp.where(band_key, band, 0.0)
        values = jnp.where(band_key, 0.0, band)
        key_sets = (keys.astype(bf16), pltpu.roll(keys, 64, 1).astype(bf16))
        value_sets = (pltpu.roll(values, 64, 1).astype(bf16), values.astype(bf16))
        allowed = in_window & (me * GROUP + n * OWN - WINDOW + key_i >= 0)
        q = qs[n]
        total = jnp.zeros((PAIRS * OWN, 128), f32)
        for odd in (0, 1):
            scores = lax.dot_general(
                q, key_sets[odd], (((1,), (1,)), ((), ())), preferred_element_type=f32
            ) * (1.0 / math.sqrt(HEAD_DIM))
            scores = jnp.where(allowed, scores, -jnp.inf)
            peak = jnp.maximum(jnp.max(scores, axis=-1, keepdims=True), sink_of[odd])
            e = jnp.exp(scores - peak)
            denominator = jnp.sum(e, axis=-1, keepdims=True) + jnp.exp(sink_of[odd] - peak)
            total = total + dot((e / denominator).astype(bf16), value_sets[odd])
        at = pl.ds(pl.multiple_of(n * OWN, OWN), OWN)
        for p in range(PAIRS):
            att[at, p * 128 : (p + 1) * 128] = total[p * OWN : (p + 1) * OWN].astype(bf16)
        return _

    lax.fori_loop(0, TP, attend, 0)

    loads["wo"].wait()

    def project_out(i, _):
        at = pl.ds(pl.multiple_of(i * OWN, OWN), OWN)
        for c in range(WIDTH // COLS):
            part = pl.ds(c * COLS, COLS)
            mix[at, part] = dot(att[at, :], wo_v[:, part]).astype(bf16)
        return _

    lax.fori_loop(0, TP, project_out, 0)

    all_blocks(out, arr, 0).wait_recv()

    def flatten(c, _):
        at = pl.ds(pl.multiple_of(c * COLS, COLS), COLS)
        rows[:, at] = arr[:, :, at].astype(f32).reshape(SLOTS, COLS).astype(bf16)
        return _

    lax.fori_loop(0, WIDTH // COLS, flatten, 0)

    def hidden(q, top=0, bottom=WIDTH):
        def body(i, _):
            at = pl.ds(pl.multiple_of(i * 256, 256), 256)
            g = dot(rows[at, top:bottom], gate[q, top:bottom, :])
            u = dot(rows[at, top:bottom], up[q, top:bottom, :])
            if top > 0:
                g, u = g + gate_sum[at, :], u + up_sum[at, :]
            if bottom < WIDTH:
                gate_sum[at, :] = g
                up_sum[at, :] = u
                return _
            hid[at, q * PART : (q + 1) * PART] = (g / (1.0 + jnp.exp(-g)) * u).astype(bf16)
            return _

        lax.fori_loop(0, SLOTS // 256, body, 0)

    loads["gate"].wait()
    loads["up"].wait()
    hidden(0)
    messages[UP_L].wait_recv()
    hidden(1)
    messages[GATE_R].wait_recv()
    hidden(2)

    foreign = pl.ds(1, TP - 1)
    messages[STRIP_FL].wait_recv()
    messages[STRIP_FR].wait_recv()

    def spread(s, _):
        peer = me - place + lax.rem(place + s, ROW)
        pltpu.make_async_remote_copy(
            src_ref=strips.at[foreign, strip], dst_ref=strips.at[foreign, strip],
            send_sem=x_send.at[1 + CHUNKS], recv_sem=x_recv.at[1 + CHUNKS],
            device_id={"ep": peer}, device_id_type=MESH,
        ).start()
        return _

    lax.fori_loop(1, ROW, spread, 0)
    others = strips.at[foreign, pl.ds(0, SHARED - STRIP)]
    all_strips = pltpu.make_async_remote_copy(
        src_ref=others, dst_ref=others, send_sem=x_send.at[1 + CHUNKS], recv_sem=x_recv.at[1 + CHUNKS],
        device_id={"ep": lax.rem(me + 1, EP)}, device_id_type=MESH,
    )

    half = PART // 2

    def forward_down(c):
        messages[DOWN_L + c].wait_recv()
        message(
            DOWN_FL + c, down[c].at[pl.ds(PART, half)], down[c].at[pl.ds(3 * PART, half)], {"tp": right}
        )
        messages[DOWN_R + c].wait_recv()
        message(
            DOWN_FR + c, down[c].at[pl.ds(2 * PART + half, half)], down[c].at[pl.ds(3 * PART + half, half)],
            {"tp": left},
        )

    forward_down(0)
    send_down(1)
    send_down(2)

    near = 3 * PART
    loads["down0"].wait()

    def begin(i, _):
        at = pl.ds(pl.multiple_of(i * 256, 256), 256)
        first_sum[at, :] = dot(hid[at, 0:near], down[0][0:near, :])
        return _

    lax.fori_loop(0, SLOTS // 256, begin, 0)
    for k in (0, 1):
        messages[GATE_F[k]].wait_recv()
        messages[UP_F[k]].wait_recv()
        hidden(3, *DEPTHS[k])

    def finish(c):
        if c > 0:
            loads[f"down{c}"].wait()
        messages[DOWN_FL + c].wait_recv()
        messages[DOWN_FR + c].wait_recv()

        def body(i, _):
            at = pl.ds(pl.multiple_of(i * 256, 256), 256)
            if c == 0:
                got = first_sum[at, :] + dot(hid[at, near:], down[0][near:, :])
            else:
                got = dot(hid[at, :], down[c][...])
            blocks = pl.ds(i * (256 // CAP), 256 // CAP)
            res[c][blocks] = got.reshape(256 // CAP, CAP, CUTS[c]).astype(bf16)
            return _

        lax.fori_loop(0, SLOTS // 256, body, 0)
        exchange(lambda peer: res[c].at[peer], ret[c].at[me], 1 + c)
        ret[c][me] = res[c][me]

    def piece(ref, owner, columns):
        return ref.at[pl.ds(pl.multiple_of(owner * OWN, OWN), OWN), columns]

    low, high = pl.ds(0, HALF), pl.ds(HALF, HALF)

    finish(0)
    forward_down(1)
    send_down(3)
    for c in range(1, CHUNKS - 1):
        forward_down(c + 1)
        if c + 3 < CHUNKS:
            send_down(c + 3)
        if c + 1 == CHUNKS - 2:
            message(UNITS_L, piece(units, right, pl.ds(0, SHARED)), units_got.at[1], {"tp": right})
            message(UNITS_R, piece(units, left, pl.ds(0, SHARED)), units_got.at[2], {"tp": left})
            message(UNITS_F, piece(units, far, pl.ds(0, SHARED)), units_got.at[3], {"tp": far})
        if c + 1 < CHUNKS - 1:
            finish(c)

    message(MIX_FL, piece(mix, far, low), mix_far.at[0], {"tp": right})
    message(MIX_FR, piece(mix, far, high), mix_far.at[1], {"tp": left})
    message(MIX_L0, piece(mix, right, high), mix_got.at[0, :, high], {"tp": right})
    message(MIX_R0, piece(mix, left, low), mix_got.at[1, :, low], {"tp": left})
    finish(CHUNKS - 2)
    finish(CHUNKS - 1)

    leaving = []

    def leave(src, dst):
        copy = pltpu.make_async_copy(src, dst, out_sem.at[len(leaving)])
        copy.start()
        leaving.append(copy)

    def combine(c):
        all_blocks(res[c], ret[c], 1 + c).wait_recv()
        got = ret[c][...].astype(f32).reshape(SLOTS, CUTS[c]).astype(bf16)
        both = dot(weights[...], got)
        at = pl.ds(STARTS[c], CUTS[c])
        expert_v[:, at] = (routed[:, at] + both[0:OWN] + both[OWN:]).astype(bf16)
        leave(expert_v.at[:, at], expert_out.at[:, at])

    all_strips.wait_recv()
    for number in (UNITS_L, UNITS_R, UNITS_F):
        messages[number].wait_recv()
    for c in range(WIDTH // COLS):
        at = pl.ds(c * COLS, COLS)
        routed[:, at] = dot(units[own, :], strips[0, :, at]) + sum(
            dot(units_got[k], strips[k, :, at]) for k in range(1, TP)
        )

    def add_into(owner, columns, extra):
        at = pl.ds(pl.multiple_of(owner * OWN, OWN), OWN)
        mix[at, columns] = (mix[at, columns].astype(f32) + extra[...].astype(f32)).astype(bf16)

    combine(0)
    messages[MIX_FL].wait_recv()
    add_into(right, low, mix_far.at[0])
    message(MIX_L1, piece(mix, right, low), mix_got.at[0, :, low], {"tp": right})
    messages[MIX_FR].wait_recv()
    add_into(left, high, mix_far.at[1])
    message(MIX_R1, piece(mix, left, high), mix_got.at[1, :, high], {"tp": left})
    for c in range(1, CHUNKS - 1):
        combine(c)

    for number in (MIX_L0, MIX_R0, MIX_L1, MIX_R1):
        messages[number].wait_recv()
    mixer_v[...] = (
        mix[own, :].astype(f32) + mix_got[0].astype(f32) + mix_got[1].astype(f32)
    ).astype(bf16)
    leave(mixer_v, mixer_out)
    combine(CHUNKS - 1)

    for copy in leaving:
        copy.wait()
    for copy in messages.values():
        copy.wait_send()
    all_blocks(out, arr, 0).wait_send()
    for c in range(CHUNKS):
        all_blocks(res[c], ret[c], 1 + c).wait_send()
    all_strips.wait_send()


def hand_on(mixer_in, expert_in, mixer_out, expert_out, held, in_sem, out_sem):
    pieces = [(mixer_in, mixer_out, 0), (expert_in, expert_out, 0), (mixer_in, mixer_out, 1), (expert_in, expert_out, 1)]
    arriving, leaving = [], []
    for k, (src, _, half) in enumerate(pieces):
        copy = pltpu.make_async_copy(src.at[pl.ds(half * 64, 64)], held.at[k], in_sem.at[k])
        copy.start()
        arriving.append(copy)
    for k, (_, dst, half) in enumerate(pieces):
        arriving[k].wait()
        copy = pltpu.make_async_copy(held.at[k], dst.at[pl.ds(half * 64, 64)], out_sem.at[k])
        copy.start()
        leaving.append(copy)
    for copy in leaving:
        copy.wait()


def local(
    mixer_input, expert_input, gain_mixer, gain_expert, query_weight, key_weight, value_weight,
    sink_logits, output_weight, expert_choice, route_weights, expert_gate, expert_up, expert_down,
    shared_gate, shared_up, shared_down,
):
    half_steps = (jnp.arange(128, dtype=jnp.int32) % (HEAD_DIM // 2)).astype(f32)
    steps = (rope_base ** (-(2.0 * half_steps) / HEAD_DIM))[None]
    hbm = pl.BlockSpec(memory_space=pltpu.HBM)
    V = pltpu.VMEM
    scratch = [
        V((GROUP, WIDTH), bf16), V((GROUP, WIDTH), bf16), V((GROUP, WIDTH), bf16), V((GROUP, WIDTH), bf16),
        V((WIDTH, 384), bf16), V((128, WIDTH), bf16), V((384, WIDTH), bf16),
        V((WIDTH, SHARED), bf16), V((WIDTH, SHARED), bf16), V((TP, SHARED, WIDTH), bf16),
        V((TP, WIDTH, PART), bf16), V((TP, WIDTH, PART), bf16),
        V((EP, CAP, WIDTH), bf16), V((EP, CAP, WIDTH), bf16), V((SLOTS, WIDTH), bf16),
        V((SLOTS, TP * PART), bf16),
        V((1, WIDTH), f32), V((1, WIDTH), f32), V((1, 2 * PAIRS), f32), V((2, GROUP), jnp.int32), V((2, GROUP), f32),
        V((1, 128), f32), V((TP, PAIRS * OWN, 128), bf16), V((WINDOW + GROUP, 128), bf16), V((GROUP, 384), bf16),
        V((GROUP, WIDTH), bf16), V((2, OWN, HALF), bf16), V((2, OWN, WIDTH), bf16),
        V((GROUP, SHARED), bf16), V((TP, OWN, SHARED), bf16), V((OWN, WIDTH), f32),
        V((2 * OWN, SLOTS), bf16), V((SLOTS, OWN), bf16),
        V((OWN, WIDTH), bf16), V((OWN, WIDTH), bf16),
        V((SLOTS, PART), f32), V((SLOTS, PART), f32), V((SLOTS, CUTS[0]), f32),
        *[V((TP * PART, cut), bf16) for cut in CUTS],
        *[V((EP, CAP, cut), bf16) for cut in CUTS],
        *[V((EP, CAP, cut), bf16) for cut in CUTS],
        pltpu.SemaphoreType.DMA((32,)), pltpu.SemaphoreType.DMA((MESSAGES,)),
        pltpu.SemaphoreType.DMA((MESSAGES,)), pltpu.SemaphoreType.DMA((2 + CHUNKS,)),
        pltpu.SemaphoreType.DMA((2 + CHUNKS,)), pltpu.SemaphoreType.DMA((1 + CHUNKS,)),
    ]
    shape = jax.ShapeDtypeStruct((OWN, WIDTH), bf16)
    done = pl.pallas_call(
        kernel,
        out_shape=(shape, shape),
        in_specs=[hbm] * 18,
        out_specs=(hbm, hbm),
        scratch_shapes=scratch,
        compiler_params=pltpu.CompilerParams(
            collective_id=0, has_side_effects=True, vmem_limit_bytes=63 * 2**20
        ),
        name="everything",
    )(
        mixer_input, expert_input, query_weight, key_weight.T, value_weight.T, output_weight,
        shared_gate, shared_up, shared_down, expert_gate[0], expert_up[0], expert_down[0],
        gain_mixer[None], gain_expert[None], sink_logits[None], expert_choice.T, route_weights.T, steps,
    )
    return pl.pallas_call(
        hand_on, out_shape=(shape, shape), in_specs=[hbm] * 2, out_specs=(hbm, hbm), name="hand_on",
        scratch_shapes=[V((4, OWN // 2, WIDTH), bf16), pltpu.SemaphoreType.DMA((4,)), pltpu.SemaphoreType.DMA((4,))],
    )(*done)


def solution(mesh):
    placed = (
        P("ep", None),
        P("ep", None),
        P(),
        P(),
        P(None, "tp"),
        P(None, "tp"),
        P(None, "tp"),
        P("tp"),
        P("tp", None),
        P("ep", None),
        P("ep", None),
        P("ep", None, "tp"),
        P("ep", None, "tp"),
        P("ep", "tp", None),
        P(None, "tp"),
        P(None, "tp"),
        P("tp", None),
    )
    return jax.shard_map(
        local,
        mesh=mesh,
        in_specs=placed,
        out_specs=(P(("ep", "tp"), None), P(("ep", "tp"), None)),
        check_vma=False,
    )
```

```python
import functools
import math

import jax
import jax.numpy as jnp
from jax import lax
from jax.experimental import pallas as pl
from jax.experimental.pallas import tpu as pltpu
from jax.sharding import PartitionSpec as P

HEAD_DIM = 64
WINDOW = 128
MESH = pl.DeviceIdType.MESH

norm_eps = 1e-06
rope_base = 500000.0

GROUP = 512
OWN = 128
WIDTH = 2048
EP = 64
CAP = 8
SLOTS = EP * CAP
PART = 256
SHARED = 128
COLS = 512
CUTS = (128, 128, 128, 128) + (256,) * 6
CHUNKS = len(CUTS)
STARTS = tuple(sum(CUTS[:c]) for c in range(CHUNKS))
ROW = 16
STRIP = SHARED // ROW
HALF = WIDTH // 2
DEPTHS = ((0, 1536), (1536, WIDTH))
PAIRS = 3
TP = 4

GATE_L, UP_L, GATE_R, UP_R, TAIL = range(5)
GATE_F, UP_F = (20 + 4 * CHUNKS, 21 + 4 * CHUNKS), (22 + 4 * CHUNKS, 23 + 4 * CHUNKS)
STRIP_L, STRIP_R, STRIP_FL, STRIP_FR, UNITS_L, UNITS_R, UNITS_F = range(7, 14)
MIX_FL, MIX_FR, MIX_L0, MIX_L1, MIX_R0, MIX_R1 = range(14, 20)
DOWN_L, DOWN_R, DOWN_FL, DOWN_FR = (20 + CHUNKS * k for k in range(4))
MESSAGES = 24 + 4 * CHUNKS

f32, bf16 = jnp.float32, jnp.bfloat16


def dot(a, b):
    return jnp.dot(a, b, preferred_element_type=f32)


def kernel(
    xa, xb, wq, wk, wv, wo, sgate, sup, sdown, gate_in, up_in, down_in,
    gain_a_in, gain_b_in, sinks_in, choice_in, route_in, steps_in,
    mixer_out, expert_out,
    xa_v, xb_v, na, nb, wq_v, wkv_v, wo_v, sg_v, su_v, sd_v, strips,
    gate, up, out, arr, rows, hid,
    gain_a, gain_b, sinks, choice_rows, route, steps,
    qs, kvx, att, mix, mix_far, mix_got, units, units_got, routed, weights, picks, mixer_v, expert_v, gate_sum, up_sum, first_sum,
    *rest,
):
    down, res, ret = (rest[k * CHUNKS : (k + 1) * CHUNKS] for k in range(3))
    load_sem, send_sem, recv_sem, x_send, x_recv, out_sem = rest[3 * CHUNKS :]
    me = lax.axis_index("ep")
    t = lax.axis_index("tp")
    right = lax.rem(t + 1, TP)
    left = lax.rem(t + TP - 1, TP)
    far = lax.rem(t + 2, TP)

    barrier = pltpu.get_barrier_semaphore()

    def greet(s, _):
        pl.semaphore_signal(barrier, inc=1, device_id={"ep": lax.rem(me + s, EP)}, device_id_type=MESH)
        return _

    for neighbour in (left, right, far):
        pl.semaphore_signal(barrier, inc=1, device_id={"tp": neighbour}, device_id_type=MESH)
    lax.fori_loop(1, EP, greet, 0)

    loads = {}

    def load(name, src, dst):
        copy = pltpu.make_async_copy(src, dst, load_sem.at[len(loads)])
        copy.start()
        loads[name] = copy

    load("choice", choice_in, choice_rows)
    load("route", route_in, route)
    load("gain_b", gain_b_in, gain_b)
    load("xb", xb, xb_v)
    load("gain_a", gain_a_in, gain_a)
    load("sinks", sinks_in, sinks)
    load("steps", steps_in, steps)
    load("sg", sgate, sg_v)
    load("su", sup, su_v)
    load("sd", sdown, sd_v)
    load("xa", xa, xa_v)
    load("wq", wq, wq_v)
    load("wk", wk, wkv_v.at[pl.ds(0, HEAD_DIM)])
    load("wv", wv, wkv_v.at[pl.ds(HEAD_DIM, HEAD_DIM)])
    load("wo", wo, wo_v)

    messages = {}

    def message(number, src, dst, to):
        copy = pltpu.make_async_remote_copy(
            src_ref=src, dst_ref=dst, send_sem=send_sem.at[number], recv_sem=recv_sem.at[number],
            device_id=to, device_id_type=MESH,
        )
        copy.start()
        messages[number] = copy

    pl.semaphore_wait(barrier, EP + 2)

    place = lax.rem(me, ROW)
    strip = pl.ds(pl.multiple_of(place * STRIP, STRIP), STRIP)
    message(STRIP_L, sdown.at[strip], strips.at[0, place], {"tp": right})
    message(STRIP_R, sdown.at[strip], strips.at[1, place], {"tp": left})
    message(GATE_L, gate_in, gate.at[1], {"tp": right})
    message(UP_R, up_in, up.at[2], {"tp": left})
    message(UP_L, up_in, up.at[1], {"tp": right})
    message(GATE_R, gate_in, gate.at[2], {"tp": left})

    def send_down(c):
        src = down_in.at[:, pl.ds(STARTS[c], CUTS[c])]
        message(DOWN_L + c, src, down[c].at[pl.ds(PART, PART)], {"tp": right})
        message(DOWN_R + c, src, down[c].at[pl.ds(2 * PART, PART)], {"tp": left})

    send_down(0)
    load("gate", gate_in, gate.at[0])
    load("up", up_in, up.at[0])
    for c in range(CHUNKS):
        load(f"down{c}", down_in.at[:, pl.ds(STARTS[c], CUTS[c])], down[c].at[pl.ds(0, PART)])

    own = pl.ds(pl.multiple_of(t * OWN, OWN), OWN)
    loads["choice"].wait()
    loads["route"].wait()
    row_a = choice_rows[0:1, own].astype(f32)
    row_b = choice_rows[1:2, own].astype(f32)
    down_i = lax.broadcasted_iota(jnp.int32, (OWN, OWN), 0)
    across_i = lax.broadcasted_iota(jnp.int32, (OWN, OWN), 1)

    def column(row):
        return jnp.sum(jnp.where(down_i == across_i, row, 0.0), axis=1, keepdims=True)

    col_a, col_b = column(row_a), column(row_b)

    def count(condition, axis):
        return jnp.sum(jnp.where(condition, 1.0, 0.0).astype(f32), axis=axis, keepdims=True)

    before = down_i < across_i
    after = down_i > across_i
    slot_row_a = row_a * CAP + count((col_a == row_a) & before, 0)
    slot_row_b = row_b * CAP + count(col_a == row_b, 0) + count((col_b == row_b) & before, 0)
    slot_col_a = col_a * CAP + count((col_a == row_a) & after, 1)
    slot_col_b = col_b * CAP + count(col_b == row_a, 1) + count((col_b == row_b) & after, 1)
    slot_i = lax.broadcasted_iota(jnp.int32, (SLOTS, OWN), 0).astype(f32)
    picks[...] = jnp.where((slot_i == slot_row_a) | (slot_i == slot_row_b), 1.0, 0.0).astype(bf16)
    slot_j = lax.broadcasted_iota(jnp.int32, (OWN, SLOTS), 1).astype(f32)
    share = jnp.where(slot_j == slot_col_a, column(route[0:1, own]), 0.0) + jnp.where(
        slot_j == slot_col_b, column(route[1:2, own]), 0.0
    )
    coarse = share.astype(bf16)
    weights[0:OWN, :] = coarse
    weights[OWN:, :] = (share - coarse.astype(f32)).astype(bf16)

    def normalise(src, dst, gain, start, count_of):
        step = 32

        def body(i, _):
            at = pl.ds(pl.multiple_of(start + i * step, step), step)
            wide = src[at, :].astype(f32)
            scale = lax.rsqrt(jnp.mean(wide * wide, axis=-1, keepdims=True) + norm_eps)
            dst[at, :] = (wide * scale * gain[...]).astype(bf16)
            return _

        lax.fori_loop(0, count_of // step, body, 0)

    loads["gain_b"].wait()
    loads["xb"].wait()
    normalise(xb_v, nb, gain_b, t * OWN, OWN)

    def gather(c, _):
        at = pl.ds(pl.multiple_of(c * COLS, COLS), COLS)
        got = dot(picks[...], nb[own, at])
        out[:, :, at] = got.reshape(EP, CAP, COLS).astype(bf16)
        return _

    lax.fori_loop(0, WIDTH // COLS, gather, 0)

    def exchange(src_of, dst, number):
        def body(s, _):
            peer = lax.rem(me + s, EP)
            pltpu.make_async_remote_copy(
                src_ref=src_of(peer), dst_ref=dst, send_sem=x_send.at[number], recv_sem=x_recv.at[number],
                device_id={"ep": peer}, device_id_type=MESH,
            ).start()
            return _

        lax.fori_loop(1, EP, body, 0)

    def all_blocks(src, dst, number):
        most = pl.ds(0, EP - 1)
        return pltpu.make_async_remote_copy(
            src_ref=src.at[most], dst_ref=dst.at[most], send_sem=x_send.at[number], recv_sem=x_recv.at[number],
            device_id={"ep": lax.rem(me + 1, EP)}, device_id_type=MESH,
        )

    exchange(lambda peer: out.at[peer], arr.at[me], 0)
    arr[me] = out[me]

    normalise(xb_v, nb, gain_b, 0, GROUP)
    for name in ("sg", "su", "sd"):
        loads[name].wait()

    def shared(i, _):
        at = pl.ds(pl.multiple_of(i * OWN, OWN), OWN)
        g = dot(nb[at, :], sg_v[...])
        u = dot(nb[at, :], su_v[...])
        units[at, :] = (g / (1.0 + jnp.exp(-g)) * u).astype(bf16)
        return _

    lax.fori_loop(0, TP, shared, 0)

    for name in ("xa", "wq", "wk", "wv", "gain_a", "sinks", "steps"):
        loads[name].wait()
    normalise(xa_v, na, gain_a, 0, GROUP)
    lane = lax.broadcasted_iota(jnp.int32, (OWN, 128), 1)
    first_half = (lane & 63) < 32
    is_key = lane < 64

    def turn(value, c, s):
        value = value.astype(bf16).astype(f32)
        partner = jnp.where(first_half, pltpu.roll(value, 96, 1), pltpu.roll(value, 32, 1))
        return (value * c + partner * s).astype(bf16)

    def project(i, _):
        at = pl.ds(pl.multiple_of(i * OWN, OWN), OWN)
        position = me * GROUP + i * OWN + down_i
        angles = position.astype(f32) * steps[...]
        c, s = jnp.cos(angles), jnp.sin(angles)
        s = jnp.where(first_half, -s, s)
        q = dot(na[at, :], wq_v[...])
        for p in range(PAIRS):
            qs[i, p * OWN : (p + 1) * OWN, :] = turn(q[:, p * 128 : (p + 1) * 128], c, s)
        kv = lax.dot_general(na[at, :], wkv_v[...], (((1,), (1,)), ((), ())), preferred_element_type=f32)
        after_tail = pl.ds(pl.multiple_of(WINDOW + i * OWN, OWN), OWN)
        kvx[after_tail, :] = turn(kv, jnp.where(is_key, c, 1.0), jnp.where(is_key, s, 0.0))
        return _

    lax.fori_loop(0, TP, project, 0)
    message(TAIL, kvx.at[pl.ds(GROUP, WINDOW)], kvx.at[pl.ds(0, WINDOW)], {"ep": lax.rem(me + 1, EP)})

    messages[STRIP_L].wait_recv()
    messages[STRIP_R].wait_recv()
    for number, k, part, to in (
        (STRIP_FL, 0, pl.ds(0, HALF), right), (STRIP_FR, 1, pl.ds(HALF, HALF), left),
    ):
        message(number, strips.at[k, place, :, part], strips.at[2, place, :, part], {"tp": to})

    messages[GATE_L].wait_recv()
    for number, (top, bottom) in zip(GATE_F, DEPTHS):
        depth = pl.ds(top, bottom - top)
        message(number, gate.at[1, depth], gate.at[3, depth], {"tp": right})
    messages[UP_R].wait_recv()
    for number, (top, bottom) in zip(UP_F, DEPTHS):
        depth = pl.ds(top, bottom - top)
        message(number, up.at[2, depth], up.at[3, depth], {"tp": left})

    messages[TAIL].wait_recv()

    band_lane = lax.broadcasted_iota(jnp.int32, (2 * WINDOW, 128), 1)
    band_key = band_lane < 64
    query_i = lax.broadcasted_iota(jnp.int32, (PAIRS * OWN, 2 * WINDOW), 0) & (WINDOW - 1)
    key_i = lax.broadcasted_iota(jnp.int32, (PAIRS * OWN, 2 * WINDOW), 1)
    distance = query_i + WINDOW - key_i
    in_window = (distance >= 0) & (distance < WINDOW)
    head_row = lax.broadcasted_iota(jnp.int32, (PAIRS * OWN, 1), 0)

    def sink(head):
        return sinks[0:1, head : head + 1]

    sink_of = [
        jnp.where(
            head_row < OWN, sink(odd), jnp.where(head_row < 2 * OWN, sink(2 + odd), sink(4 + odd))
        )
        for odd in (0, 1)
    ]

    def attend(n, _):
        band = kvx[pl.ds(pl.multiple_of(n * OWN, OWN), 2 * WINDOW), :].astype(f32)
        keys = jnp.where(band_key, band, 0.0)
        values = jnp.where(band_key, 0.0, band)
        key_sets = (keys.astype(bf16), pltpu.roll(keys, 64, 1).astype(bf16))
        value_sets = (pltpu.roll(values, 64, 1).astype(bf16), values.astype(bf16))
        allowed = in_window & (me * GROUP + n * OWN - WINDOW + key_i >= 0)
        q = qs[n]
        total = jnp.zeros((PAIRS * OWN, 128), f32)
        for odd in (0, 1):
            scores = lax.dot_general(
                q, key_sets[odd], (((1,), (1,)), ((), ())), preferred_element_type=f32
            ) * (1.0 / math.sqrt(HEAD_DIM))
            scores = jnp.where(allowed, scores, -jnp.inf)
            peak = jnp.maximum(jnp.max(scores, axis=-1, keepdims=True), sink_of[odd])
            e = jnp.exp(scores - peak)
            denominator = jnp.sum(e, axis=-1, keepdims=True) + jnp.exp(sink_of[odd] - peak)
            total = total + dot((e / denominator).astype(bf16), value_sets[odd])
        at = pl.ds(pl.multiple_of(n * OWN, OWN), OWN)
        for p in range(PAIRS):
            att[at, p * 128 : (p + 1) * 128] = total[p * OWN : (p + 1) * OWN].astype(bf16)
        return _

    lax.fori_loop(0, TP, attend, 0)

    loads["wo"].wait()

    def project_out(i, _):
        at = pl.ds(pl.multiple_of(i * OWN, OWN), OWN)
        for c in range(WIDTH // COLS):
            part = pl.ds(c * COLS, COLS)
            mix[at, part] = dot(att[at, :], wo_v[:, part]).astype(bf16)
        return _

    lax.fori_loop(0, TP, project_out, 0)

    all_blocks(out, arr, 0).wait_recv()

    def flatten(c, _):
        at = pl.ds(pl.multiple_of(c * COLS, COLS), COLS)
        rows[:, at] = arr[:, :, at].astype(f32).reshape(SLOTS, COLS).astype(bf16)
        return _

    lax.fori_loop(0, WIDTH // COLS, flatten, 0)

    def hidden(q, top=0, bottom=WIDTH):
        def body(i, _):
            at = pl.ds(pl.multiple_of(i * 256, 256), 256)
            g = dot(rows[at, top:bottom], gate[q, top:bottom, :])
            u = dot(rows[at, top:bottom], up[q, top:bottom, :])
            if top > 0:
                g, u = g + gate_sum[at, :], u + up_sum[at, :]
            if bottom < WIDTH:
                gate_sum[at, :] = g
                up_sum[at, :] = u
                return _
            hid[at, q * PART : (q + 1) * PART] = (g / (1.0 + jnp.exp(-g)) * u).astype(bf16)
            return _

        lax.fori_loop(0, SLOTS // 256, body, 0)

    loads["gate"].wait()
    loads["up"].wait()
    hidden(0)
    messages[UP_L].wait_recv()
    hidden(1)
    messages[GATE_R].wait_recv()
    hidden(2)

    foreign = pl.ds(0, TP - 1)
    messages[STRIP_FL].wait_recv()
    messages[STRIP_FR].wait_recv()

    def spread(s, _):
        peer = me - place + lax.rem(place + s, ROW)
        pltpu.make_async_remote_copy(
            src_ref=strips.at[foreign, place], dst_ref=strips.at[foreign, place],
            send_sem=x_send.at[1 + CHUNKS], recv_sem=x_recv.at[1 + CHUNKS],
            device_id={"ep": peer}, device_id_type=MESH,
        ).start()
        return _

    lax.fori_loop(1, ROW, spread, 0)
    others = strips.at[foreign, pl.ds(0, ROW - 1)]
    all_strips = pltpu.make_async_remote_copy(
        src_ref=others, dst_ref=others, send_sem=x_send.at[1 + CHUNKS], recv_sem=x_recv.at[1 + CHUNKS],
        device_id={"ep": lax.rem(me + 1, EP)}, device_id_type=MESH,
    )

    half = PART // 2

    def forward_down(c):
        messages[DOWN_L + c].wait_recv()
        message(
            DOWN_FL + c, down[c].at[pl.ds(PART, half)], down[c].at[pl.ds(3 * PART, half)], {"tp": right}
        )
        messages[DOWN_R + c].wait_recv()
        message(
            DOWN_FR + c, down[c].at[pl.ds(2 * PART + half, half)], down[c].at[pl.ds(3 * PART + half, half)],
            {"tp": left},
        )

    forward_down(0)
    send_down(1)
    send_down(2)

    near = 3 * PART
    loads["down0"].wait()

    def begin(i, _):
        at = pl.ds(pl.multiple_of(i * 256, 256), 256)
        first_sum[at, :] = dot(hid[at, 0:near], down[0][0:near, :])
        return _

    lax.fori_loop(0, SLOTS // 256, begin, 0)
    for k in (0, 1):
        messages[GATE_F[k]].wait_recv()
        messages[UP_F[k]].wait_recv()
        hidden(3, *DEPTHS[k])

    def finish(c):
        if c > 0:
            loads[f"down{c}"].wait()
        messages[DOWN_FL + c].wait_recv()
        messages[DOWN_FR + c].wait_recv()

        def body(i, _):
            at = pl.ds(pl.multiple_of(i * 256, 256), 256)
            if c == 0:
                got = first_sum[at, :] + dot(hid[at, near:], down[0][near:, :])
            else:
                got = dot(hid[at, :], down[c][...])
            blocks = pl.ds(i * (256 // CAP), 256 // CAP)
            res[c][blocks] = got.reshape(256 // CAP, CAP, CUTS[c]).astype(bf16)
            return _

        lax.fori_loop(0, SLOTS // 256, body, 0)
        exchange(lambda peer: res[c].at[peer], ret[c].at[me], 1 + c)
        ret[c][me] = res[c][me]

    def piece(ref, owner, columns):
        return ref.at[pl.ds(pl.multiple_of(owner * OWN, OWN), OWN), columns]

    low, high = pl.ds(0, HALF), pl.ds(HALF, HALF)

    finish(0)
    forward_down(1)
    send_down(3)
    for c in range(1, CHUNKS - 1):
        forward_down(c + 1)
        if c + 3 < CHUNKS:
            send_down(c + 3)
        if c + 1 == CHUNKS - 2:
            message(UNITS_L, piece(units, right, pl.ds(0, SHARED)), units_got.at[1], {"tp": right})
            message(UNITS_R, piece(units, left, pl.ds(0, SHARED)), units_got.at[2], {"tp": left})
            message(UNITS_F, piece(units, far, pl.ds(0, SHARED)), units_got.at[3], {"tp": far})
        if c + 1 < CHUNKS - 1:
            finish(c)

    message(MIX_FL, piece(mix, far, low), mix_far.at[0], {"tp": right})
    message(MIX_FR, piece(mix, far, high), mix_far.at[1], {"tp": left})
    message(MIX_L0, piece(mix, right, high), mix_got.at[0, :, high], {"tp": right})
    message(MIX_R0, piece(mix, left, low), mix_got.at[1, :, low], {"tp": left})
    finish(CHUNKS - 2)
    finish(CHUNKS - 1)

    leaving = []

    def leave(src, dst):
        copy = pltpu.make_async_copy(src, dst, out_sem.at[len(leaving)])
        copy.start()
        leaving.append(copy)

    def combine(c):
        all_blocks(res[c], ret[c], 1 + c).wait_recv()
        got = ret[c][...].astype(f32).reshape(SLOTS, CUTS[c]).astype(bf16)
        both = dot(weights[...], got)
        at = pl.ds(STARTS[c], CUTS[c])
        expert_v[:, at] = (routed[:, at] + both[0:OWN] + both[OWN:]).astype(bf16)
        leave(expert_v.at[:, at], expert_out.at[:, at])

    all_strips.wait_recv()
    for number in (UNITS_L, UNITS_R, UNITS_F):
        messages[number].wait_recv()
    for c in range(WIDTH // COLS):
        at = pl.ds(c * COLS, COLS)
        routed[:, at] = dot(units[own, :], sd_v[:, at]) + sum(
            dot(units_got[k], strips[k - 1, :, :, at].astype(f32).reshape(SHARED, COLS).astype(bf16))
            for k in range(1, TP)
        )

    def add_into(owner, columns, extra):
        at = pl.ds(pl.multiple_of(owner * OWN, OWN), OWN)
        mix[at, columns] = (mix[at, columns].astype(f32) + extra[...].astype(f32)).astype(bf16)

    combine(0)
    messages[MIX_FL].wait_recv()
    add_into(right, low, mix_far.at[0])
    message(MIX_L1, piece(mix, right, low), mix_got.at[0, :, low], {"tp": right})
    messages[MIX_FR].wait_recv()
    add_into(left, high, mix_far.at[1])
    message(MIX_R1, piece(mix, left, high), mix_got.at[1, :, high], {"tp": left})
    for c in range(1, CHUNKS - 1):
        combine(c)

    for number in (MIX_L0, MIX_R0, MIX_L1, MIX_R1):
        messages[number].wait_recv()
    mixer_v[...] = (
        mix[own, :].astype(f32) + mix_got[0].astype(f32) + mix_got[1].astype(f32)
    ).astype(bf16)
    leave(mixer_v, mixer_out)
    combine(CHUNKS - 1)

    for copy in leaving:
        copy.wait()
    for copy in messages.values():
        copy.wait_send()
    all_blocks(out, arr, 0).wait_send()
    for c in range(CHUNKS):
        all_blocks(res[c], ret[c], 1 + c).wait_send()
    all_strips.wait_send()


def hand_on(mixer_in, expert_in, mixer_out, expert_out, held, in_sem, out_sem):
    pieces = [(mixer_in, mixer_out, 0), (expert_in, expert_out, 0), (mixer_in, mixer_out, 1), (expert_in, expert_out, 1)]
    arriving, leaving = [], []
    for k, (src, _, half) in enumerate(pieces):
        copy = pltpu.make_async_copy(src.at[pl.ds(half * 64, 64)], held.at[k], in_sem.at[k])
        copy.start()
        arriving.append(copy)
    for k, (_, dst, half) in enumerate(pieces):
        arriving[k].wait()
        copy = pltpu.make_async_copy(held.at[k], dst.at[pl.ds(half * 64, 64)], out_sem.at[k])
        copy.start()
        leaving.append(copy)
    for copy in leaving:
        copy.wait()


def local(
    mixer_input, expert_input, gain_mixer, gain_expert, query_weight, key_weight, value_weight,
    sink_logits, output_weight, expert_choice, route_weights, expert_gate, expert_up, expert_down,
    shared_gate, shared_up, shared_down,
):
    half_steps = (jnp.arange(128, dtype=jnp.int32) % (HEAD_DIM // 2)).astype(f32)
    steps = (rope_base ** (-(2.0 * half_steps) / HEAD_DIM))[None]
    hbm = pl.BlockSpec(memory_space=pltpu.HBM)
    V = pltpu.VMEM
    scratch = [
        V((GROUP, WIDTH), bf16), V((GROUP, WIDTH), bf16), V((GROUP, WIDTH), bf16), V((GROUP, WIDTH), bf16),
        V((WIDTH, 384), bf16), V((128, WIDTH), bf16), V((384, WIDTH), bf16),
        V((WIDTH, SHARED), bf16), V((WIDTH, SHARED), bf16), V((SHARED, WIDTH), bf16), V((TP - 1, ROW, STRIP, WIDTH), bf16),
        V((TP, WIDTH, PART), bf16), V((TP, WIDTH, PART), bf16),
        V((EP, CAP, WIDTH), bf16), V((EP, CAP, WIDTH), bf16), V((SLOTS, WIDTH), bf16),
        V((SLOTS, TP * PART), bf16),
        V((1, WIDTH), f32), V((1, WIDTH), f32), V((1, 2 * PAIRS), f32), V((2, GROUP), jnp.int32), V((2, GROUP), f32),
        V((1, 128), f32), V((TP, PAIRS * OWN, 128), bf16), V((WINDOW + GROUP, 128), bf16), V((GROUP, 384), bf16),
        V((GROUP, WIDTH), bf16), V((2, OWN, HALF), bf16), V((2, OWN, WIDTH), bf16),
        V((GROUP, SHARED), bf16), V((TP, OWN, SHARED), bf16), V((OWN, WIDTH), f32),
        V((2 * OWN, SLOTS), bf16), V((SLOTS, OWN), bf16),
        V((OWN, WIDTH), bf16), V((OWN, WIDTH), bf16),
        V((SLOTS, PART), f32), V((SLOTS, PART), f32), V((SLOTS, CUTS[0]), f32),
        *[V((TP * PART, cut), bf16) for cut in CUTS],
        *[V((EP, CAP, cut), bf16) for cut in CUTS],
        *[V((EP, CAP, cut), bf16) for cut in CUTS],
        pltpu.SemaphoreType.DMA((32,)), pltpu.SemaphoreType.DMA((MESSAGES,)),
        pltpu.SemaphoreType.DMA((MESSAGES,)), pltpu.SemaphoreType.DMA((2 + CHUNKS,)),
        pltpu.SemaphoreType.DMA((2 + CHUNKS,)), pltpu.SemaphoreType.DMA((1 + CHUNKS,)),
    ]
    shape = jax.ShapeDtypeStruct((OWN, WIDTH), bf16)
    done = pl.pallas_call(
        kernel,
        out_shape=(shape, shape),
        in_specs=[hbm] * 18,
        out_specs=(hbm, hbm),
        scratch_shapes=scratch,
        compiler_params=pltpu.CompilerParams(
            collective_id=0, has_side_effects=True, vmem_limit_bytes=63 * 2**20
        ),
        name="everything",
    )(
        mixer_input, expert_input, query_weight, key_weight.T, value_weight.T, output_weight,
        shared_gate, shared_up, shared_down, expert_gate[0], expert_up[0], expert_down[0],
        gain_mixer[None], gain_expert[None], sink_logits[None], expert_choice.T, route_weights.T, steps,
    )
    return pl.pallas_call(
        hand_on, out_shape=(shape, shape), in_specs=[hbm] * 2, out_specs=(hbm, hbm), name="hand_on",
        scratch_shapes=[V((4, OWN // 2, WIDTH), bf16), pltpu.SemaphoreType.DMA((4,)), pltpu.SemaphoreType.DMA((4,))],
    )(*done)


def solution(mesh):
    placed = (
        P("ep", None),
        P("ep", None),
        P(),
        P(),
        P(None, "tp"),
        P(None, "tp"),
        P(None, "tp"),
        P("tp"),
        P("tp", None),
        P("ep", None),
        P("ep", None),
        P("ep", None, "tp"),
        P("ep", None, "tp"),
        P("ep", "tp", None),
        P(None, "tp"),
        P(None, "tp"),
        P("tp", None),
    )
    return jax.shard_map(
        local,
        mesh=mesh,
        in_specs=placed,
        out_specs=(P(("ep", "tp"), None), P(("ep", "tp"), None)),
        check_vma=False,
    )
```

```python
import functools
import math

import jax
import jax.numpy as jnp
from jax import lax
from jax.experimental import pallas as pl
from jax.experimental.pallas import tpu as pltpu
from jax.sharding import PartitionSpec as P

HEAD_DIM = 64
WINDOW = 128
MESH = pl.DeviceIdType.MESH

norm_eps = 1e-06
rope_base = 500000.0

GROUP = 512
OWN = 128
WIDTH = 2048
EP = 64
CAP = 8
SLOTS = EP * CAP
PART = 256
SHARED = 128
COLS = 512
CUTS = (128, 128, 128, 128) + (256,) * 4 + (512,)
CHUNKS = len(CUTS)
STARTS = tuple(sum(CUTS[:c]) for c in range(CHUNKS))
ROW = 16
STRIP = SHARED // ROW
HALF = WIDTH // 2
DEPTHS = ((0, 1792), (1792, WIDTH))
PAIRS = 3
TP = 4

GATE_L, UP_L, GATE_R, UP_R, TAIL = range(5)
GATE_F, UP_F = (20 + 4 * CHUNKS, 21 + 4 * CHUNKS), (22 + 4 * CHUNKS, 23 + 4 * CHUNKS)
STRIP_L, STRIP_R, STRIP_FL, STRIP_FR, UNITS_L, UNITS_R, UNITS_F = range(7, 14)
MIX_FL, MIX_FR, MIX_L0, MIX_L1, MIX_R0, MIX_R1 = range(14, 20)
DOWN_L, DOWN_R, DOWN_FL, DOWN_FR = (20 + CHUNKS * k for k in range(4))
MESSAGES = 24 + 4 * CHUNKS

f32, bf16 = jnp.float32, jnp.bfloat16


def dot(a, b):
    return jnp.dot(a, b, preferred_element_type=f32)


def kernel(
    xa, xb, wq, wk, wv, wo, sgate, sup, sdown, gate_in, up_in, down_in,
    gain_a_in, gain_b_in, sinks_in, choice_in, route_in, steps_in,
    mixer_out, expert_out,
    xa_v, xb_v, na, nb, wq_v, wkv_v, wo_v, sg_v, su_v, sd_v, strips,
    gate, up, out, arr, rows, hid,
    gain_a, gain_b, sinks, choice_rows, route, steps,
    qs, kvx, att, mix, mix_far, mix_got, units, units_got, routed, weights, picks, mixer_v, expert_v, gate_sum, up_sum, first_sum,
    *rest,
):
    down, res, ret = (rest[k * CHUNKS : (k + 1) * CHUNKS] for k in range(3))
    load_sem, send_sem, recv_sem, x_send, x_recv, out_sem = rest[3 * CHUNKS :]
    me = lax.axis_index("ep")
    t = lax.axis_index("tp")
    right = lax.rem(t + 1, TP)
    left = lax.rem(t + TP - 1, TP)
    far = lax.rem(t + 2, TP)

    barrier = pltpu.get_barrier_semaphore()

    def greet(s, _):
        pl.semaphore_signal(barrier, inc=1, device_id={"ep": lax.rem(me + s, EP)}, device_id_type=MESH)
        return _

    for neighbour in (left, right, far):
        pl.semaphore_signal(barrier, inc=1, device_id={"tp": neighbour}, device_id_type=MESH)
    lax.fori_loop(1, EP, greet, 0)

    loads = {}

    def load(name, src, dst):
        copy = pltpu.make_async_copy(src, dst, load_sem.at[len(loads)])
        copy.start()
        loads[name] = copy

    load("choice", choice_in, choice_rows)
    load("route", route_in, route)
    load("gain_b", gain_b_in, gain_b)
    load("xb", xb, xb_v)
    load("gain_a", gain_a_in, gain_a)
    load("sinks", sinks_in, sinks)
    load("steps", steps_in, steps)
    load("sg", sgate, sg_v)
    load("su", sup, su_v)
    load("sd", sdown, sd_v)
    load("xa", xa, xa_v)
    load("wq", wq, wq_v)
    load("wk", wk, wkv_v.at[pl.ds(0, HEAD_DIM)])
    load("wv", wv, wkv_v.at[pl.ds(HEAD_DIM, HEAD_DIM)])
    load("wo", wo, wo_v)

    messages = {}

    def message(number, src, dst, to):
        copy = pltpu.make_async_remote_copy(
            src_ref=src, dst_ref=dst, send_sem=send_sem.at[number], recv_sem=recv_sem.at[number],
            device_id=to, device_id_type=MESH,
        )
        copy.start()
        messages[number] = copy

    pl.semaphore_wait(barrier, EP + 2)

    place = lax.rem(me, ROW)
    strip = pl.ds(pl.multiple_of(place * STRIP, STRIP), STRIP)
    message(STRIP_L, sdown.at[strip], strips.at[0, place], {"tp": right})
    message(STRIP_R, sdown.at[strip], strips.at[1, place], {"tp": left})
    message(GATE_L, gate_in, gate.at[1], {"tp": right})
    message(UP_R, up_in, up.at[2], {"tp": left})
    message(UP_L, up_in, up.at[1], {"tp": right})
    message(GATE_R, gate_in, gate.at[2], {"tp": left})

    def send_down(c):
        src = down_in.at[:, pl.ds(STARTS[c], CUTS[c])]
        message(DOWN_L + c, src, down[c].at[pl.ds(PART, PART)], {"tp": right})
        message(DOWN_R + c, src, down[c].at[pl.ds(2 * PART, PART)], {"tp": left})

    send_down(0)
    load("gate", gate_in, gate.at[0])
    load("up", up_in, up.at[0])
    for c in range(CHUNKS):
        load(f"down{c}", down_in.at[:, pl.ds(STARTS[c], CUTS[c])], down[c].at[pl.ds(0, PART)])

    own = pl.ds(pl.multiple_of(t * OWN, OWN), OWN)
    loads["choice"].wait()
    loads["route"].wait()
    row_a = choice_rows[0:1, own].astype(f32)
    row_b = choice_rows[1:2, own].astype(f32)
    down_i = lax.broadcasted_iota(jnp.int32, (OWN, OWN), 0)
    across_i = lax.broadcasted_iota(jnp.int32, (OWN, OWN), 1)

    def column(row):
        return jnp.sum(jnp.where(down_i == across_i, row, 0.0), axis=1, keepdims=True)

    col_a, col_b = column(row_a), column(row_b)

    def count(condition, axis):
        return jnp.sum(jnp.where(condition, 1.0, 0.0).astype(f32), axis=axis, keepdims=True)

    before = down_i < across_i
    after = down_i > across_i
    slot_row_a = row_a * CAP + count((col_a == row_a) & before, 0)
    slot_row_b = row_b * CAP + count(col_a == row_b, 0) + count((col_b == row_b) & before, 0)
    slot_col_a = col_a * CAP + count((col_a == row_a) & after, 1)
    slot_col_b = col_b * CAP + count(col_b == row_a, 1) + count((col_b == row_b) & after, 1)
    slot_i = lax.broadcasted_iota(jnp.int32, (SLOTS, OWN), 0).astype(f32)
    picks[...] = jnp.where((slot_i == slot_row_a) | (slot_i == slot_row_b), 1.0, 0.0).astype(bf16)
    slot_j = lax.broadcasted_iota(jnp.int32, (OWN, SLOTS), 1).astype(f32)
    share = jnp.where(slot_j == slot_col_a, column(route[0:1, own]), 0.0) + jnp.where(
        slot_j == slot_col_b, column(route[1:2, own]), 0.0
    )
    coarse = share.astype(bf16)
    weights[0:OWN, :] = coarse
    weights[OWN:, :] = (share - coarse.astype(f32)).astype(bf16)

    def normalise(src, dst, gain, start, count_of):
        step = 32

        def body(i, _):
            at = pl.ds(pl.multiple_of(start + i * step, step), step)
            wide = src[at, :].astype(f32)
            scale = lax.rsqrt(jnp.mean(wide * wide, axis=-1, keepdims=True) + norm_eps)
            dst[at, :] = (wide * scale * gain[...]).astype(bf16)
            return _

        lax.fori_loop(0, count_of // step, body, 0)

    loads["gain_b"].wait()
    loads["xb"].wait()
    normalise(xb_v, nb, gain_b, t * OWN, OWN)

    def gather(c, _):
        at = pl.ds(pl.multiple_of(c * COLS, COLS), COLS)
        got = dot(picks[...], nb[own, at])
        out[:, :, at] = got.reshape(EP, CAP, COLS).astype(bf16)
        return _

    lax.fori_loop(0, WIDTH // COLS, gather, 0)

    def exchange(src_of, dst, number):
        def body(s, _):
            peer = lax.rem(me + s, EP)
            pltpu.make_async_remote_copy(
                src_ref=src_of(peer), dst_ref=dst, send_sem=x_send.at[number], recv_sem=x_recv.at[number],
                device_id={"ep": peer}, device_id_type=MESH,
            ).start()
            return _

        lax.fori_loop(1, EP, body, 0)

    def all_blocks(src, dst, number):
        most = pl.ds(0, EP - 1)
        return pltpu.make_async_remote_copy(
            src_ref=src.at[most], dst_ref=dst.at[most], send_sem=x_send.at[number], recv_sem=x_recv.at[number],
            device_id={"ep": lax.rem(me + 1, EP)}, device_id_type=MESH,
        )

    exchange(lambda peer: out.at[peer], arr.at[me], 0)
    arr[me] = out[me]

    normalise(xb_v, nb, gain_b, 0, GROUP)
    for name in ("sg", "su", "sd"):
        loads[name].wait()

    def shared(i, _):
        at = pl.ds(pl.multiple_of(i * OWN, OWN), OWN)
        g = dot(nb[at, :], sg_v[...])
        u = dot(nb[at, :], su_v[...])
        units[at, :] = (g / (1.0 + jnp.exp(-g)) * u).astype(bf16)
        return _

    lax.fori_loop(0, TP, shared, 0)

    for name in ("xa", "wq", "wk", "wv", "gain_a", "sinks", "steps"):
        loads[name].wait()
    normalise(xa_v, na, gain_a, 0, GROUP)
    lane = lax.broadcasted_iota(jnp.int32, (OWN, 128), 1)
    first_half = (lane & 63) < 32
    is_key = lane < 64

    def turn(value, c, s):
        value = value.astype(bf16).astype(f32)
        partner = jnp.where(first_half, pltpu.roll(value, 96, 1), pltpu.roll(value, 32, 1))
        return (value * c + partner * s).astype(bf16)

    def project(i, _):
        at = pl.ds(pl.multiple_of(i * OWN, OWN), OWN)
        position = me * GROUP + i * OWN + down_i
        angles = position.astype(f32) * steps[...]
        c, s = jnp.cos(angles), jnp.sin(angles)
        s = jnp.where(first_half, -s, s)
        q = dot(na[at, :], wq_v[...])
        for p in range(PAIRS):
            qs[i, p * OWN : (p + 1) * OWN, :] = turn(q[:, p * 128 : (p + 1) * 128], c, s)
        kv = lax.dot_general(na[at, :], wkv_v[...], (((1,), (1,)), ((), ())), preferred_element_type=f32)
        after_tail = pl.ds(pl.multiple_of(WINDOW + i * OWN, OWN), OWN)
        kvx[after_tail, :] = turn(kv, jnp.where(is_key, c, 1.0), jnp.where(is_key, s, 0.0))
        return _

    lax.fori_loop(0, TP, project, 0)
    message(TAIL, kvx.at[pl.ds(GROUP, WINDOW)], kvx.at[pl.ds(0, WINDOW)], {"ep": lax.rem(me + 1, EP)})

    messages[STRIP_L].wait_recv()
    messages[STRIP_R].wait_recv()
    for number, k, part, to in (
        (STRIP_FL, 0, pl.ds(0, HALF), right), (STRIP_FR, 1, pl.ds(HALF, HALF), left),
    ):
        message(number, strips.at[k, place, :, part], strips.at[2, place, :, part], {"tp": to})

    messages[GATE_L].wait_recv()
    for number, (top, bottom) in zip(GATE_F, DEPTHS):
        depth = pl.ds(top, bottom - top)
        message(number, gate.at[1, depth], gate.at[3, depth], {"tp": right})
    messages[UP_R].wait_recv()
    for number, (top, bottom) in zip(UP_F, DEPTHS):
        depth = pl.ds(top, bottom - top)
        message(number, up.at[2, depth], up.at[3, depth], {"tp": left})

    messages[TAIL].wait_recv()

    band_lane = lax.broadcasted_iota(jnp.int32, (2 * WINDOW, 128), 1)
    band_key = band_lane < 64
    query_i = lax.broadcasted_iota(jnp.int32, (PAIRS * OWN, 2 * WINDOW), 0) & (WINDOW - 1)
    key_i = lax.broadcasted_iota(jnp.int32, (PAIRS * OWN, 2 * WINDOW), 1)
    distance = query_i + WINDOW - key_i
    in_window = (distance >= 0) & (distance < WINDOW)
    head_row = lax.broadcasted_iota(jnp.int32, (PAIRS * OWN, 1), 0)

    def sink(head):
        return sinks[0:1, head : head + 1]

    sink_of = [
        jnp.where(
            head_row < OWN, sink(odd), jnp.where(head_row < 2 * OWN, sink(2 + odd), sink(4 + odd))
        )
        for odd in (0, 1)
    ]

    def attend(n, _):
        band = kvx[pl.ds(pl.multiple_of(n * OWN, OWN), 2 * WINDOW), :].astype(f32)
        keys = jnp.where(band_key, band, 0.0)
        values = jnp.where(band_key, 0.0, band)
        key_sets = (keys.astype(bf16), pltpu.roll(keys, 64, 1).astype(bf16))
        value_sets = (pltpu.roll(values, 64, 1).astype(bf16), values.astype(bf16))
        allowed = in_window & (me * GROUP + n * OWN - WINDOW + key_i >= 0)
        q = qs[n]
        total = jnp.zeros((PAIRS * OWN, 128), f32)
        for odd in (0, 1):
            scores = lax.dot_general(
                q, key_sets[odd], (((1,), (1,)), ((), ())), preferred_element_type=f32
            ) * (1.0 / math.sqrt(HEAD_DIM))
            scores = jnp.where(allowed, scores, -jnp.inf)
            peak = jnp.maximum(jnp.max(scores, axis=-1, keepdims=True), sink_of[odd])
            e = jnp.exp(scores - peak)
            denominator = jnp.sum(e, axis=-1, keepdims=True) + jnp.exp(sink_of[odd] - peak)
            total = total + dot((e / denominator).astype(bf16), value_sets[odd])
        at = pl.ds(pl.multiple_of(n * OWN, OWN), OWN)
        for p in range(PAIRS):
            att[at, p * 128 : (p + 1) * 128] = total[p * OWN : (p + 1) * OWN].astype(bf16)
        return _

    lax.fori_loop(0, TP, attend, 0)

    loads["wo"].wait()

    def project_out(i, _):
        at = pl.ds(pl.multiple_of(i * OWN, OWN), OWN)
        for c in range(WIDTH // COLS):
            part = pl.ds(c * COLS, COLS)
            mix[at, part] = dot(att[at, :], wo_v[:, part]).astype(bf16)
        return _

    lax.fori_loop(0, TP, project_out, 0)

    all_blocks(out, arr, 0).wait_recv()

    def flatten(c, _):
        at = pl.ds(pl.multiple_of(c * COLS, COLS), COLS)
        rows[:, at] = arr[:, :, at].astype(f32).reshape(SLOTS, COLS).astype(bf16)
        return _

    lax.fori_loop(0, WIDTH // COLS, flatten, 0)

    def hidden(q, top=0, bottom=WIDTH):
        def body(i, _):
            at = pl.ds(pl.multiple_of(i * 256, 256), 256)
            g = dot(rows[at, top:bottom], gate[q, top:bottom, :])
            u = dot(rows[at, top:bottom], up[q, top:bottom, :])
            if top > 0:
                g, u = g + gate_sum[at, :], u + up_sum[at, :]
            if bottom < WIDTH:
                gate_sum[at, :] = g
                up_sum[at, :] = u
                return _
            hid[at, q * PART : (q + 1) * PART] = (g / (1.0 + jnp.exp(-g)) * u).astype(bf16)
            return _

        lax.fori_loop(0, SLOTS // 256, body, 0)

    loads["gate"].wait()
    loads["up"].wait()
    hidden(0)
    messages[UP_L].wait_recv()
    hidden(1)
    messages[GATE_R].wait_recv()
    hidden(2)

    foreign = pl.ds(0, TP - 1)
    messages[STRIP_FL].wait_recv()
    messages[STRIP_FR].wait_recv()

    def spread(s, _):
        peer = me - place + lax.rem(place + s, ROW)
        pltpu.make_async_remote_copy(
            src_ref=strips.at[foreign, place], dst_ref=strips.at[foreign, place],
            send_sem=x_send.at[1 + CHUNKS], recv_sem=x_recv.at[1 + CHUNKS],
            device_id={"ep": peer}, device_id_type=MESH,
        ).start()
        return _

    lax.fori_loop(1, ROW, spread, 0)
    others = strips.at[foreign, pl.ds(0, ROW - 1)]
    all_strips = pltpu.make_async_remote_copy(
        src_ref=others, dst_ref=others, send_sem=x_send.at[1 + CHUNKS], recv_sem=x_recv.at[1 + CHUNKS],
        device_id={"ep": lax.rem(me + 1, EP)}, device_id_type=MESH,
    )

    half = PART // 2

    def forward_down(c):
        messages[DOWN_L + c].wait_recv()
        message(
            DOWN_FL + c, down[c].at[pl.ds(PART, half)], down[c].at[pl.ds(3 * PART, half)], {"tp": right}
        )
        messages[DOWN_R + c].wait_recv()
        message(
            DOWN_FR + c, down[c].at[pl.ds(2 * PART + half, half)], down[c].at[pl.ds(3 * PART + half, half)],
            {"tp": left},
        )

    forward_down(0)
    send_down(1)
    send_down(2)

    near = 3 * PART
    loads["down0"].wait()

    def begin(i, _):
        at = pl.ds(pl.multiple_of(i * 256, 256), 256)
        first_sum[at, :] = dot(hid[at, 0:near], down[0][0:near, :])
        return _

    lax.fori_loop(0, SLOTS // 256, begin, 0)
    for k in (0, 1):
        messages[GATE_F[k]].wait_recv()
        messages[UP_F[k]].wait_recv()
        hidden(3, *DEPTHS[k])

    def finish(c):
        if c > 0:
            loads[f"down{c}"].wait()
        messages[DOWN_FL + c].wait_recv()
        messages[DOWN_FR + c].wait_recv()

        def body(i, _):
            at = pl.ds(pl.multiple_of(i * 256, 256), 256)
            if c == 0:
                got = first_sum[at, :] + dot(hid[at, near:], down[0][near:, :])
            else:
                got = dot(hid[at, :], down[c][...])
            blocks = pl.ds(i * (256 // CAP), 256 // CAP)
            res[c][blocks] = got.reshape(256 // CAP, CAP, CUTS[c]).astype(bf16)
            return _

        lax.fori_loop(0, SLOTS // 256, body, 0)
        exchange(lambda peer: res[c].at[peer], ret[c].at[me], 1 + c)
        ret[c][me] = res[c][me]

    def piece(ref, owner, columns):
        return ref.at[pl.ds(pl.multiple_of(owner * OWN, OWN), OWN), columns]

    low, high = pl.ds(0, HALF), pl.ds(HALF, HALF)

    finish(0)
    forward_down(1)
    send_down(3)
    for c in range(1, CHUNKS - 1):
        forward_down(c + 1)
        if c + 3 < CHUNKS:
            send_down(c + 3)
        if c + 1 == CHUNKS - 2:
            message(UNITS_L, piece(units, right, pl.ds(0, SHARED)), units_got.at[1], {"tp": right})
            message(UNITS_R, piece(units, left, pl.ds(0, SHARED)), units_got.at[2], {"tp": left})
            message(UNITS_F, piece(units, far, pl.ds(0, SHARED)), units_got.at[3], {"tp": far})
        if c + 1 < CHUNKS - 1:
            finish(c)

    message(MIX_FL, piece(mix, far, low), mix_far.at[0], {"tp": right})
    message(MIX_FR, piece(mix, far, high), mix_far.at[1], {"tp": left})
    message(MIX_L0, piece(mix, right, high), mix_got.at[0, :, high], {"tp": right})
    message(MIX_R0, piece(mix, left, low), mix_got.at[1, :, low], {"tp": left})
    finish(CHUNKS - 2)
    finish(CHUNKS - 1)

    leaving = []

    def leave(src, dst):
        copy = pltpu.make_async_copy(src, dst, out_sem.at[len(leaving)])
        copy.start()
        leaving.append(copy)

    def combine(c):
        all_blocks(res[c], ret[c], 1 + c).wait_recv()
        got = ret[c][...].astype(f32).reshape(SLOTS, CUTS[c]).astype(bf16)
        both = dot(weights[...], got)
        at = pl.ds(STARTS[c], CUTS[c])
        expert_v[:, at] = (routed[:, at] + both[0:OWN] + both[OWN:]).astype(bf16)
        leave(expert_v.at[:, at], expert_out.at[:, at])

    all_strips.wait_recv()
    for number in (UNITS_L, UNITS_R, UNITS_F):
        messages[number].wait_recv()
    for c in range(WIDTH // COLS):
        at = pl.ds(c * COLS, COLS)
        routed[:, at] = dot(units[own, :], sd_v[:, at]) + sum(
            dot(units_got[k], strips[k - 1, :, :, at].astype(f32).reshape(SHARED, COLS).astype(bf16))
            for k in range(1, TP)
        )

    def add_into(owner, columns, extra):
        at = pl.ds(pl.multiple_of(owner * OWN, OWN), OWN)
        mix[at, columns] = (mix[at, columns].astype(f32) + extra[...].astype(f32)).astype(bf16)

    combine(0)
    messages[MIX_FL].wait_recv()
    add_into(right, low, mix_far.at[0])
    message(MIX_L1, piece(mix, right, low), mix_got.at[0, :, low], {"tp": right})
    messages[MIX_FR].wait_recv()
    add_into(left, high, mix_far.at[1])
    message(MIX_R1, piece(mix, left, high), mix_got.at[1, :, high], {"tp": left})
    for c in range(1, CHUNKS - 1):
        combine(c)

    for number in (MIX_L0, MIX_R0, MIX_L1, MIX_R1):
        messages[number].wait_recv()
    mixer_v[...] = (
        mix[own, :].astype(f32) + mix_got[0].astype(f32) + mix_got[1].astype(f32)
    ).astype(bf16)
    leave(mixer_v, mixer_out)
    combine(CHUNKS - 1)

    for copy in leaving:
        copy.wait()
    for copy in messages.values():
        copy.wait_send()
    all_blocks(out, arr, 0).wait_send()
    for c in range(CHUNKS):
        all_blocks(res[c], ret[c], 1 + c).wait_send()
    all_strips.wait_send()


def hand_on(mixer_in, expert_in, mixer_out, expert_out, held, in_sem, out_sem):
    pieces = [(mixer_in, mixer_out, 0), (expert_in, expert_out, 0), (mixer_in, mixer_out, 1), (expert_in, expert_out, 1)]
    arriving, leaving = [], []
    for k, (src, _, half) in enumerate(pieces):
        copy = pltpu.make_async_copy(src.at[pl.ds(half * 64, 64)], held.at[k], in_sem.at[k])
        copy.start()
        arriving.append(copy)
    for k, (_, dst, half) in enumerate(pieces):
        arriving[k].wait()
        copy = pltpu.make_async_copy(held.at[k], dst.at[pl.ds(half * 64, 64)], out_sem.at[k])
        copy.start()
        leaving.append(copy)
    for copy in leaving:
        copy.wait()


def local(
    mixer_input, expert_input, gain_mixer, gain_expert, query_weight, key_weight, value_weight,
    sink_logits, output_weight, expert_choice, route_weights, expert_gate, expert_up, expert_down,
    shared_gate, shared_up, shared_down,
):
    half_steps = (jnp.arange(128, dtype=jnp.int32) % (HEAD_DIM // 2)).astype(f32)
    steps = (rope_base ** (-(2.0 * half_steps) / HEAD_DIM))[None]
    hbm = pl.BlockSpec(memory_space=pltpu.HBM)
    V = pltpu.VMEM
    scratch = [
        V((GROUP, WIDTH), bf16), V((GROUP, WIDTH), bf16), V((GROUP, WIDTH), bf16), V((GROUP, WIDTH), bf16),
        V((WIDTH, 384), bf16), V((128, WIDTH), bf16), V((384, WIDTH), bf16),
        V((WIDTH, SHARED), bf16), V((WIDTH, SHARED), bf16), V((SHARED, WIDTH), bf16), V((TP - 1, ROW, STRIP, WIDTH), bf16),
        V((TP, WIDTH, PART), bf16), V((TP, WIDTH, PART), bf16),
        V((EP, CAP, WIDTH), bf16), V((EP, CAP, WIDTH), bf16), V((SLOTS, WIDTH), bf16),
        V((SLOTS, TP * PART), bf16),
        V((1, WIDTH), f32), V((1, WIDTH), f32), V((1, 2 * PAIRS), f32), V((2, GROUP), jnp.int32), V((2, GROUP), f32),
        V((1, 128), f32), V((TP, PAIRS * OWN, 128), bf16), V((WINDOW + GROUP, 128), bf16), V((GROUP, 384), bf16),
        V((GROUP, WIDTH), bf16), V((2, OWN, HALF), bf16), V((2, OWN, WIDTH), bf16),
        V((GROUP, SHARED), bf16), V((TP, OWN, SHARED), bf16), V((OWN, WIDTH), f32),
        V((2 * OWN, SLOTS), bf16), V((SLOTS, OWN), bf16),
        V((OWN, WIDTH), bf16), V((OWN, WIDTH), bf16),
        V((SLOTS, PART), f32), V((SLOTS, PART), f32), V((SLOTS, CUTS[0]), f32),
        *[V((TP * PART, cut), bf16) for cut in CUTS],
        *[V((EP, CAP, cut), bf16) for cut in CUTS],
        *[V((EP, CAP, cut), bf16) for cut in CUTS],
        pltpu.SemaphoreType.DMA((32,)), pltpu.SemaphoreType.DMA((MESSAGES,)),
        pltpu.SemaphoreType.DMA((MESSAGES,)), pltpu.SemaphoreType.DMA((2 + CHUNKS,)),
        pltpu.SemaphoreType.DMA((2 + CHUNKS,)), pltpu.SemaphoreType.DMA((1 + CHUNKS,)),
    ]
    shape = jax.ShapeDtypeStruct((OWN, WIDTH), bf16)
    done = pl.pallas_call(
        kernel,
        out_shape=(shape, shape),
        in_specs=[hbm] * 18,
        out_specs=(hbm, hbm),
        scratch_shapes=scratch,
        compiler_params=pltpu.CompilerParams(
            collective_id=0, has_side_effects=True, vmem_limit_bytes=63 * 2**20
        ),
        name="everything",
    )(
        mixer_input, expert_input, query_weight, key_weight.T, value_weight.T, output_weight,
        shared_gate, shared_up, shared_down, expert_gate[0], expert_up[0], expert_down[0],
        gain_mixer[None], gain_expert[None], sink_logits[None], expert_choice.T, route_weights.T, steps,
    )
    return pl.pallas_call(
        hand_on, out_shape=(shape, shape), in_specs=[hbm] * 2, out_specs=(hbm, hbm), name="hand_on",
        scratch_shapes=[V((4, OWN // 2, WIDTH), bf16), pltpu.SemaphoreType.DMA((4,)), pltpu.SemaphoreType.DMA((4,))],
    )(*done)


def solution(mesh):
    placed = (
        P("ep", None),
        P("ep", None),
        P(),
        P(),
        P(None, "tp"),
        P(None, "tp"),
        P(None, "tp"),
        P("tp"),
        P("tp", None),
        P("ep", None),
        P("ep", None),
        P("ep", None, "tp"),
        P("ep", None, "tp"),
        P("ep", "tp", None),
        P(None, "tp"),
        P(None, "tp"),
        P("tp", None),
    )
    return jax.shard_map(
        local,
        mesh=mesh,
        in_specs=placed,
        out_specs=(P(("ep", "tp"), None), P(("ep", "tp"), None)),
        check_vma=False,
    )
```
